32 devices in a mesh: grp: 2 (over y), fs: 4 (over z), tp: 4 (over x, core).
Axes of the slice: x: 2, y: 2, z: 4, core: 2. Of those that a mesh axis runs over, the one named last changes fastest.
Arguments:
- tokens: bfloat16 [4096, 2048], P(('grp', 'fs', 'tp')), parts along dimension 0, may hold values from -6 to 6
- route_ids: int32 [4096, 8], P(('grp', 'fs', 'tp')), parts along dimension 0, may hold values from 0 to 15, all different within a row; in each aligned block of 128 rows (0 to 127, 128 to 255, ...) at most 96 rows name the same one
- route_scores: float32 [4096, 8], P(('grp', 'fs', 'tp')), parts along dimension 0, may hold values from 0.05 to 1
- norm_gain: float32 [2048], P('fs'), may hold values from 0.1 to 1.9
- expert_gate: float32 [16, 2048, 256], P(None, 'fs', 'tp'), may hold values from -0.125 to 0.125
- expert_up: float32 [16, 2048, 256], P(None, 'fs', 'tp'), may hold values from -0.125 to 0.125
- expert_down: float32 [16, 256, 2048], P(None, 'fs', 'tp'), may hold values from -0.375 to 0.375
- shared_gate: float32 [2048, 256], P('fs', 'tp'), may hold values from -0.125 to 0.125
- shared_up: float32 [2048, 256], P('fs', 'tp'), may hold values from -0.125 to 0.125
- shared_down: float32 [256, 2048], P('fs', 'tp'), may hold values from -0.375 to 0.375
Outputs:
- mixed: bfloat16 [4096, 2048], P(('grp', 'fs', 'tp')), parts along dimension 0
- sampler_gate: bfloat16 [32, 2048, 256], P(('grp', 'fs', 'tp')), parts along dimension 0
- sampler_up: bfloat16 [32, 2048, 256], P(('grp', 'fs', 'tp')), parts along dimension 0
- sampler_down: bfloat16 [32, 256, 2048], P(('grp', 'fs', 'tp')), parts along dimension 0
- sampler_shared_gate: bfloat16 [4096, 256], P(('grp', 'fs')), parts along dimension 0
- sampler_shared_up: bfloat16 [4096, 256], P(('grp', 'fs')), parts along dimension 0
- sampler_shared_down: bfloat16 [512, 2048], P(('grp', 'fs')), parts along dimension 0
The draws below stay inside these ranges and needn't reach their ends.
There are 2 independent parts, one for each index of `grp`. The reference program is written for one: setup_inputs(seed, part) draws one part's arguments, and reference() takes and returns one part's arrays. A program takes and returns all parts, laid end to end along the dimension named above; an argument that names none is the same for every part. Nothing has to cross between parts.
Inputs may be any that keep to these rules, and one draw needn't show every extreme that they name: `route_ids`: each row names 8 different experts. Among the 128 rows of one device no expert is named more than 96 times, a bound that some block reaches.
All inputs are finite; a program needn't handle non-finite values.
Results may differ from the reference program's by a relative error of at most 0.0084.
Values may be sent and summed in bfloat16 or wider, within the bound.
A program may use at most 128 MiB of HBM per device.

```python
import math
import jax
import jax.numpy as jnp
import numpy as np
from jax import lax

D = 2048
F = 256
SH = 256
TOP_K = 8
TOK_DEV = 128
EXPERTS = 16
TOKENS = 2048
CAP = 96


def level_of(rng, extent, pieces, least, largest):
    def one(dim, blocks):
        draws = jax.random.uniform(jax.random.fold_in(jax.random.fold_in(rng, 6), dim), (blocks,), jnp.float32, least / len(pieces), largest / len(pieces))
        return jnp.repeat(jnp.exp(draws), extent[dim] // blocks).reshape((-1,) + (1,) * (len(extent) - dim - 1))

    factor_of = one(*pieces[0])
    for cut in pieces[1:]:
        factor_of = factor_of * one(*cut)
    return factor_of


def routed_block(own_key, own, number, rows, number_of, top, most, skew):
    ranking = jax.random.permutation(own_key, number_of)
    packed, usual = shares(number_of, rows * top, most, skew, True), shares(number_of, rows * top, most, skew, False)
    places = jnp.arange(number_of)

    def named(tallies, rotation):
        used = int((tallies > 0).sum())
        fixed = max(1, used // 4)
        moved = fixed + (places - fixed + rotation * (used - fixed)) % max(1, number_of - fixed)
        return jnp.zeros((number_of,), jnp.int32).at[ranking[jnp.where(places < fixed, places, moved)]].set(jnp.asarray(tallies, jnp.int32))

    tallies = jnp.where(number % 4 == 0, named(packed, number // 4), named(usual, number - number // 4 - 1))
    mixed = jax.random.permutation(jax.random.fold_in(own, 3), number_of)
    giver, taker = mixed[0:number_of // 2 * 2:2], mixed[1:number_of // 2 * 2:2]
    slack = jnp.minimum(tallies[giver] - 1, most - tallies[taker]) // 2
    slack = jnp.where((giver == ranking[0]) | (taker == ranking[0]) | (tallies[taker] == 0), 0, jnp.maximum(slack, 0))
    moved = jax.random.randint(jax.random.fold_in(own, 4), (number_of // 2,), 0, 1 << 20) % (slack + 1)
    tallies = tallies.at[giver].add(-moved).at[taker].add(moved)
    items = jnp.searchsorted(jnp.cumsum(tallies), jnp.arange(rows * top), side="right").astype(jnp.int32)
    listing = items.reshape(top, rows).T
    listing = listing[jax.random.permutation(jax.random.fold_in(own, 1), rows)]
    rotation = jax.random.randint(jax.random.fold_in(own, 2), (rows, 1), 0, top)
    return jnp.take_along_axis(listing, (jnp.arange(top)[None, :] + rotation) % top, axis=1)


def shares(amount, total, most, slope, full):
    weights = [(1 << 20) // math.isqrt(grade ** slope) + 1 for grade in range(1, amount + 1)]
    largest = most if full else min(most, max(-(-total // amount), total * weights[0] // sum(weights)))
    least = 1 if total - largest >= amount - 1 else 0
    given, surplus = [largest] + [least] * (amount - 1), total - largest - least * (amount - 1)
    while surplus > 0:
        movable = [i for i in range(1, amount) if given[i] < largest] or [i for i in range(1, amount) if given[i] < most]
        whole, left = sum([weights[i] for i in movable]), surplus
        for i in movable:
            addition = min(most - given[i], max(1, left * weights[i] // whole), surplus)
            given[i] = given[i] + addition
            surplus = surplus - addition
    return np.array(given)


def bell_draw(stream_key, shape, width, bound, pieces=(), held_as=jnp.bfloat16):
    result = jax.random.normal(stream_key, shape, jnp.float32) * width
    if len(pieces) > 0:
        result = level_of(stream_key, shape, pieces, -0.22, 0.18) * result
    return jnp.clip(result, min=-bound, max=bound).astype(held_as)


def setup_inputs(seed: int = 0, part: int = 0) -> dict:
    arg_keys = jax.random.split(jax.random.key(seed), 11)
    part_keys = jax.random.split(jax.random.fold_in(arg_keys[10], part), 11)
    tokens = bell_draw(part_keys[0], (TOKENS, D), 1.0, 6.0, ((0, 16),))
    route_ids_keys = jax.random.split(jax.random.fold_in(part_keys[1], 1), TOKENS // TOK_DEV)
    route_ids_turns = jax.random.permutation(jax.random.fold_in(part_keys[1], 3), TOKENS // TOK_DEV)
    route_ids = jax.vmap(lambda own, number: routed_block(jax.random.fold_in(part_keys[1], 2), own, number, TOK_DEV, EXPERTS, TOP_K, CAP, 1))(route_ids_keys, route_ids_turns).reshape((TOKENS, TOP_K))
    route_scores = jnp.clip(0.05 + 0.95 * jax.random.uniform(part_keys[2], (TOKENS, TOP_K), jnp.float32) ** level_of(part_keys[2], (TOKENS, TOP_K), ((0, 16),), -0.2, 0.2), 0.05, 1.0)
    norm_gain = jnp.clip(1.0 + 0.18 * jax.random.normal(arg_keys[3], (D,), jnp.float32), 0.1, 1.9)
    expert_gate = bell_draw(arg_keys[4], (EXPERTS, D, F), D ** -0.5, 0.125, ((1, 4), (2, 4)), jnp.float32)
    expert_up = bell_draw(arg_keys[5], (EXPERTS, D, F), D ** -0.5, 0.125, ((1, 4), (2, 4)), jnp.float32)
    expert_down = bell_draw(arg_keys[6], (EXPERTS, F, D), F ** -0.5, 0.375, ((1, 4), (2, 4)), jnp.float32)
    shared_gate = bell_draw(arg_keys[7], (D, SH), D ** -0.5, 0.125, ((0, 4), (1, 4)), jnp.float32)
    shared_up = bell_draw(arg_keys[8], (D, SH), D ** -0.5, 0.125, ((0, 4), (1, 4)), jnp.float32)
    shared_down = bell_draw(arg_keys[9], (SH, D), SH ** -0.5, 0.375, ((0, 4), (1, 4)), jnp.float32)
    return {"tokens": tokens, "route_ids": route_ids, "route_scores": route_scores, "norm_gain": norm_gain, "expert_gate": expert_gate, "expert_up": expert_up, "expert_down": expert_down, "shared_gate": shared_gate, "shared_up": shared_up, "shared_down": shared_down}


EPSILON = 1e-06
route_scale = 2.5

def reference(tokens, route_ids, route_scores, norm_gain, expert_gate, expert_up, expert_down, shared_gate, shared_up, shared_down):
    gain_col = norm_gain[:, None]
    sampler_gate = (gain_col[None] * expert_gate).astype(jnp.bfloat16)
    sampler_up = (gain_col[None] * expert_up).astype(jnp.bfloat16)
    sampler_down = expert_down.astype(jnp.bfloat16)
    sampler_shared_gate = (gain_col * shared_gate).astype(jnp.bfloat16)
    sampler_shared_up = (gain_col * shared_up).astype(jnp.bfloat16)
    sampler_shared_down = shared_down.astype(jnp.bfloat16)
    widened = tokens.astype(jnp.float32)
    normed = (widened * lax.rsqrt(lax.optimization_barrier(jnp.mean(widened * widened, axis=1, keepdims=True)) + EPSILON)).astype(jnp.bfloat16)
    weights = route_scale * route_scores / lax.optimization_barrier(jnp.sum(route_scores, axis=1, keepdims=True))
    gate_part = jnp.dot(normed, sampler_shared_gate, preferred_element_type=jnp.float32)
    up_part = jnp.dot(normed, sampler_shared_up, preferred_element_type=jnp.float32)
    shared_hidden = (jax.nn.silu(gate_part) * up_part).astype(jnp.bfloat16)
    shared_term = jnp.dot(shared_hidden, sampler_shared_down, preferred_element_type=jnp.float32)
    flat_ids = route_ids.reshape(-1)
    flat_weights = weights.reshape(-1)
    slots = EXPERTS * CAP

    def one_expert(expert, totals):
        matches = flat_ids == expert
        picked = jnp.nonzero(matches, size=slots, fill_value=0)[0].astype(jnp.int32)
        filled = (jnp.arange(slots, dtype=jnp.int32) < jnp.sum(matches.astype(jnp.int32))).astype(jnp.float32)
        owners = (picked // TOP_K).astype(jnp.int32)
        row_block = normed[owners]
        w_gate = lax.dynamic_index_in_dim(sampler_gate, expert, 0, keepdims=False)
        w_up = lax.dynamic_index_in_dim(sampler_up, expert, 0, keepdims=False)
        w_down = lax.dynamic_index_in_dim(sampler_down, expert, 0, keepdims=False)
        gate_rows = jnp.dot(row_block, w_gate, preferred_element_type=jnp.float32)
        up_rows = jnp.dot(row_block, w_up, preferred_element_type=jnp.float32)
        hidden = (jax.nn.silu(gate_rows) * up_rows).astype(jnp.bfloat16)
        produced = jnp.dot(hidden, w_down, preferred_element_type=jnp.float32).astype(jnp.bfloat16)
        factor = flat_weights[picked] * filled
        return totals.at[owners].add(produced.astype(jnp.float32) * factor[:, None])
    routed = lax.fori_loop(0, EXPERTS, one_expert, jnp.zeros(tokens.shape, jnp.float32))
    mixed = (routed + shared_term).astype(jnp.bfloat16)
    return (mixed, sampler_gate, sampler_up, sampler_down, sampler_shared_gate, sampler_shared_up, sampler_shared_down)
```

```python
import functools
import jax
import jax.numpy as jnp
from jax import lax
from jax.experimental import pallas as pl
from jax.experimental.pallas import tpu as pltpu
from jax.sharding import PartitionSpec as P

EPSILON = 1e-06
route_scale = 2.5
CORES = 2
MESH = pl.DeviceIdType.MESH


def expert_rows(row_block, w_gate, w_up, w_down):
    gate_rows = jnp.dot(row_block, w_gate, preferred_element_type=jnp.float32)
    up_rows = jnp.dot(row_block, w_up, preferred_element_type=jnp.float32)
    hidden = (jax.nn.silu(gate_rows) * up_rows).astype(jnp.bfloat16)
    return jnp.dot(hidden, w_down, preferred_element_type=jnp.float32).astype(jnp.bfloat16)


def relayout(arrived, fs_count, tp_count):
    tile_rows = arrived.shape[2]
    tile_cols = arrived.shape[3]
    grid = arrived.reshape(fs_count, tp_count, tile_rows, tile_cols)
    grid = jnp.transpose(grid, (0, 2, 1, 3))
    return grid.reshape(1, fs_count * tile_rows, tp_count * tile_cols)


def dispatch_plan(
    tokens,
    route_ids,
    route_scores,
    norm_gain,
    expert_gate,
    expert_up,
    expert_down,
    shared_gate,
    shared_up,
    shared_down,
):
    fs_count = lax.axis_size("fs")
    tp_count = lax.axis_size("tp")
    experts = fs_count * tp_count
    gain_col = norm_gain[:, None]
    piece_gate = (gain_col[None] * expert_gate).astype(jnp.bfloat16)
    piece_up = (gain_col[None] * expert_up).astype(jnp.bfloat16)
    piece_down = expert_down.astype(jnp.bfloat16)
    moved = (
        lax.all_to_all(piece_gate[:, None], ("fs", "tp"), split_axis=0, concat_axis=1, tiled=True),
        lax.all_to_all(piece_up[:, None], ("fs", "tp"), split_axis=0, concat_axis=1, tiled=True),
        lax.all_to_all(piece_down[:, None], ("fs", "tp"), split_axis=0, concat_axis=1, tiled=True),
    )
    served_gate = relayout(moved[0], fs_count, tp_count)
    served_up = relayout(moved[1], fs_count, tp_count)
    served_down = relayout(moved[2], fs_count, tp_count)
    tile_gate = (gain_col * shared_gate).astype(jnp.bfloat16)
    tile_up = (gain_col * shared_up).astype(jnp.bfloat16)
    tile_down = shared_down.astype(jnp.bfloat16)
    held_gate, held_up, held_down = (
        lax.all_gather(tile_gate, "tp", axis=1, tiled=True),
        lax.all_gather(tile_up, "tp", axis=1, tiled=True),
        lax.all_gather(tile_down, "tp", axis=1, tiled=True),
    )
    rows_dev = tokens.shape[0]
    width = tokens.shape[1]
    picks = route_ids.shape[1]
    capacity = 3 * rows_dev * picks // (2 * experts)
    widened = tokens.astype(jnp.float32)
    normed = (
        widened * lax.rsqrt(jnp.mean(widened * widened, axis=1, keepdims=True) + EPSILON)
    ).astype(jnp.bfloat16)
    weights = route_scale * route_scores / jnp.sum(route_scores, axis=1, keepdims=True)
    flat_ids = route_ids.reshape(-1)
    onehot = (flat_ids[:, None] == jnp.arange(experts, dtype=jnp.int32)[None, :]).astype(jnp.int32)
    earlier = jnp.cumsum(onehot, axis=0) - onehot
    ranks = jnp.sum(earlier * onehot, axis=1)
    target = flat_ids * capacity + ranks
    outbox = (
        jnp.zeros((experts * capacity, width), jnp.bfloat16)
        .at[target]
        .set(jnp.repeat(normed, picks, axis=0))
    )
    arrived = lax.all_to_all(
        outbox.reshape(experts, capacity, width),
        ("fs", "tp"),
        split_axis=0,
        concat_axis=0,
        tiled=True,
    )
    finished = expert_rows(
        arrived.reshape(-1, width), served_gate[0], served_up[0], served_down[0]
    ).reshape(arrived.shape)
    returned = lax.all_to_all(finished, ("fs", "tp"), split_axis=0, concat_axis=0, tiled=True)
    results = returned.reshape(experts * capacity, width)[target]
    routed = jnp.sum(
        results.reshape(rows_dev, picks, width).astype(jnp.float32) * weights[:, :, None], axis=1
    )
    columns = normed
    gate_part = jnp.dot(
        columns,
        lax.all_gather(held_gate, "fs", axis=0, tiled=True),
        preferred_element_type=jnp.float32,
    )
    up_part = jnp.dot(
        columns,
        lax.all_gather(held_up, "fs", axis=0, tiled=True),
        preferred_element_type=jnp.float32,
    )
    shared_hidden = (jax.nn.silu(gate_part) * up_part).astype(jnp.bfloat16)
    columns = shared_hidden
    shared_term = jnp.dot(
        columns,
        lax.all_gather(held_down, "fs", axis=0, tiled=True),
        preferred_element_type=jnp.float32,
    )
    mixed = (routed + shared_term).astype(jnp.bfloat16)
    return (mixed, served_gate, served_up, served_down, held_gate, held_up, held_down)


def handover_kernel(
    nz,
    nt,
    normed,
    gu,
    dn,
    sgu,
    sdn,
    shares,
    o_mix,
    o_w,
    o_hgu,
    o_hd,
    w,
    tok,
    part,
    rd,
    rx,
    rz,
    share,
    hgu,
    hd,
    mix,
    lsem,
    wsend,
    wrecv,
    ysend,
    yrecv,
    shsend,
    shrecv,
    ssend,
    srecv,
    hsend,
    hrecv,
    asend,
    arecv,
    rdsend,
    rdrecv,
    rxsend,
    rxrecv,
    rzsend,
    rzrecv,
):
    n = nz * nt
    xc = nt // CORES
    g = lax.axis_index("grp")
    z = lax.axis_index("fs")
    t = lax.axis_index("tp")
    x = t // CORES
    c = t % CORES
    me = z * nt + t
    rows, width = normed.shape
    ft, dt = gu.shape[2], gu.shape[3]
    fr, dc = dn.shape[1], dn.shape[2]
    inner = o_w.shape[1]
    sd = w.shape[1] - inner
    half_f, half_r = ft // 2, fr // 2

    def dev(zz, tt, gg=None):
        return {"grp": g if gg is None else gg, "fs": zz, "tp": tt}

    def rem(src, dst, ssem, rsem, device):
        return pltpu.make_async_remote_copy(
            src_ref=src,
            dst_ref=dst,
            send_sem=ssem,
            recv_sem=rsem,
            device_id=device,
            device_id_type=MESH,
        )

    def al(v, m):
        return pl.multiple_of(v, m)

    partner = dev(z, x * CORES + 1 - c)
    across = dev(z, t, 1 - g)

    def xdev(k):
        return dev(z, lax.rem(x + k, xc) * CORES + c)

    def slot(p, h, xb):
        return p * nt + h * xc + xb

    barrier = pltpu.get_barrier_semaphore()

    @pl.loop(1, n)
    def _(k):
        j = lax.rem(me + k, n)
        pl.semaphore_signal(barrier, 1, device_id=dev(j // nt, j % nt), device_id_type=MESH)

    pl.semaphore_signal(barrier, 1, device_id=across, device_id_type=MESH)
    pl.semaphore_wait(barrier, n)

    def gu_at(src):
        zs, ts = src // nt, src % nt
        return lambda gg: w.at[
            pl.ds(0, 2), pl.ds(al(ts * ft + gg * half_f, half_f), half_f), pl.ds(al(zs * dt, dt), dt)
        ]

    def dn_at(src):
        zs, ts = src // nt, src % nt
        return lambda gg: w.at[
            2, pl.ds(al(zs * fr + gg * half_r, half_r), half_r), pl.ds(al(ts * dc, dc), dc)
        ]

    def w_send(j):
        device = dev(j // nt, j % nt)
        return (
            rem(
                gu.at[j, pl.ds(0, 2), pl.ds(al(g * half_f, half_f), half_f), :],
                gu_at(me)(g),
                wsend.at[0, j],
                wrecv.at[0, me],
                device,
            ),
            rem(
                dn.at[j, pl.ds(al(g * half_r, half_r), half_r), :],
                dn_at(me)(g),
                wsend.at[1, j],
                wrecv.at[1, me],
                device,
            ),
        )

    def w_across(s, gg):
        return (
            rem(gu_at(s)(gg), gu_at(s)(gg), ysend.at[0, s], yrecv.at[0, s], across),
            rem(dn_at(s)(gg), dn_at(s)(gg), ysend.at[1, s], yrecv.at[1, s], across),
        )

    def share_send(j):
        return rem(
            shares.at[j], share.at[me], shsend.at[j], shrecv.at[me], dev(j // nt, j % nt)
        )

    def sgu_at(zs):
        return w.at[pl.ds(0, 2), pl.ds(inner, sd), pl.ds(al(zs * dt, dt), dt)]

    def sdn_at(ts):
        return w.at[2, pl.ds(inner, sd), pl.ds(al(ts * dc, dc), dc)]

    def sgu_send(k):
        j = t * nz + k
        return j, rem(
            sgu.at[pl.ds(0, 2), pl.ds(k * sd, sd), :],
            sgu_at(z),
            ssend.at[0, k],
            srecv.at[0, z],
            dev(j // nt, j % nt),
        )

    def sdn_send(k):
        j = z * nt + k
        return j, rem(
            sdn.at[pl.ds(k * sd, sd), :],
            sdn_at(t),
            ssend.at[1, k],
            srecv.at[1, t],
            dev(j // nt, j % nt),
        )

    def hgu_at(ts):
        return hgu.at[pl.ds(0, 2), pl.ds(al(ts * ft, ft), ft), :]

    def hd_at(ts):
        return hd.at[:, pl.ds(al(ts * dc, dc), dc)]

    def held_x(k):
        return (
            rem(sgu, hgu_at(t), hsend.at[0, k], hrecv.at[0, t], xdev(k)),
            rem(sdn, hd_at(t), hsend.at[1, k], hrecv.at[1, t], xdev(k)),
        )

    def held_core(xb):
        ts = xb * CORES + c
        return (
            rem(hgu_at(ts), hgu_at(ts), hsend.at[2, xb], hrecv.at[0, ts], partner),
            rem(hd_at(ts), hd_at(ts), hsend.at[3, xb], hrecv.at[1, ts], partner),
        )

    def a_z(p, up):
        s = slot(p, c, x)
        return rem(
            tok.at[s],
            tok.at[s],
            asend.at[0 if up else 1, s],
            arecv.at[s],
            dev(z + 1 if up else z - 1, t),
        )

    def a_x(p, k):
        s = slot(p, c, x)
        return rem(tok.at[s], tok.at[s], asend.at[2 + k, s], arecv.at[s], xdev(k))

    def a_core(p, xb):
        s = slot(p, c, xb)
        return rem(tok.at[s], tok.at[s], asend.at[2, s], arecv.at[s], partner)

    def a_wait(s):
        rem(tok.at[s], tok.at[s], asend.at[2, s], arecv.at[s], partner).wait_recv()

    def r_core(p):
        return rem(
            part.at[pl.ds(slot(p, 1 - c, 0), xc)],
            rd.at[pl.ds(p * xc, xc)],
            rdsend.at[p],
            rdrecv.at[p],
            partner,
        )

    def r_x(p, k):
        xb = lax.rem(x + k, xc)
        return rem(
            part.at[slot(p, c, xb)],
            rx.at[p * (xc - 1) + k - 1],
            rxsend.at[p, k - 1],
            rxrecv.at[p, k - 1],
            xdev(k),
        )

    def r_z(p):
        return rem(
            part.at[slot(p, c, x)], rz.at[z], rzsend.at[p], rzrecv.at[z], dev(p, t)
        )

    own = slot(z, c, x)
    locals_ = [
        pltpu.make_async_copy(normed, tok.at[own], lsem.at[0]),
        pltpu.make_async_copy(
            gu.at[me],
            w.at[pl.ds(0, 2), pl.ds(al(t * ft, ft), ft), pl.ds(al(z * dt, dt), dt)],
            lsem.at[1],
        ),
        pltpu.make_async_copy(
            dn.at[me],
            w.at[2, pl.ds(al(z * fr, fr), fr), pl.ds(al(t * dc, dc), dc)],
            lsem.at[2],
        ),
        pltpu.make_async_copy(sgu, hgu_at(t), lsem.at[3]),
        pltpu.make_async_copy(sdn, hd_at(t), lsem.at[4]),
        pltpu.make_async_copy(shares.at[me], share.at[me], lsem.at[5]),
    ]
    for cp in locals_:
        cp.start()
    self_gu = pltpu.make_async_copy(
        sgu.at[pl.ds(0, 2), pl.ds(al((me % nz) * sd, sd), sd), :], sgu_at(z), lsem.at[6]
    )
    self_dn = pltpu.make_async_copy(
        sdn.at[pl.ds(al((me % nt) * sd, sd), sd), :], sdn_at(t), lsem.at[7]
    )

    @pl.when(me // nz == t)
    def _():
        self_gu.start()

    @pl.when(me // nt == z)
    def _():
        self_dn.start()

    @pl.loop(1, n)
    def _(k):
        j = lax.rem(me + k, n)
        for cp in w_send(j):
            cp.start()
        share_send(j).start()

    for send, count in ((sgu_send, nz), (sdn_send, nt)):
        for k in range(count):
            j, cp = send(k)

            @pl.when(j != me)
            def _():
                cp.start()

    for cp in locals_:
        cp.wait()
    a_core(z, x).start()

    @pl.when(z < nz - 1)
    def _():
        a_z(z, True).start()

    @pl.when(z > 0)
    def _():
        a_z(z, False).start()

    for k in range(1, xc):
        a_x(z, k).start()

    @pl.loop(1, n)
    def _(k):
        s = lax.rem(me + n - k, n)
        for i, at in ((0, gu_at), (1, dn_at)):
            rem(at(s)(g), at(s)(g), ysend.at[i, s], wrecv.at[i, s], across).wait_recv()
        for cp in w_across(s, g):
            cp.start()

    @pl.loop(1, n)
    def _(k):
        s = lax.rem(me + n - k, n)
        for cp in w_across(s, 1 - g):
            cp.wait_recv()
        rem(shares.at[s], share.at[s], shsend.at[s], shrecv.at[s], across).wait_recv()

    for k in range(nz):
        @pl.when(k * nt + me // nz != me)
        def _():
            rem(sgu_at(k), sgu_at(k), ssend.at[0, k], srecv.at[0, k], across).wait_recv()

    for k in range(nt):
        @pl.when((me // nt) * nt + k != me)
        def _():
            rem(sdn_at(k), sdn_at(k), ssend.at[1, k], srecv.at[1, k], across).wait_recv()

    @pl.when(me // nz == t)
    def _():
        self_gu.wait()

    @pl.when(me // nt == z)
    def _():
        self_dn.wait()

    outs = [pltpu.make_async_copy(w.at[:, pl.ds(0, inner), :], o_w, lsem.at[0])]
    outs[0].start()

    nt_dims = (((1,), (1,)), ((), ()))

    def compute(p, h):
        first = slot(p, h, 0)
        xs = tok[pl.ds(first, xc)].reshape(xc * rows, width)
        gate = lax.dot_general(xs, w[0], nt_dims, preferred_element_type=jnp.float32)
        up = lax.dot_general(xs, w[1], nt_dims, preferred_element_type=jnp.float32)
        hidden = gate / (1.0 + jnp.exp(-gate)) * up
        scale = jnp.concatenate(
            [
                jnp.transpose(jnp.broadcast_to(share[p * nt + xb * CORES + h], (rows, rows)))
                for xb in range(xc)
            ],
            axis=0,
        )[:, :1]
        col = lax.broadcasted_iota(jnp.int32, hidden.shape, 1)
        hidden = jnp.where(col < inner, hidden * scale, hidden).astype(jnp.bfloat16)
        step = min(512, width)
        for lo in range(0, width, step):
            res = jnp.dot(hidden, w[2, :, lo : lo + step], preferred_element_type=jnp.float32)
            part[pl.ds(first, xc), :, lo : lo + step] = res.astype(jnp.bfloat16).reshape(
                xc, rows, step
            )

    steps = 2 * nz - 1

    def plane(i):
        d = (i + 1) // 2
        p = z + d * (1 - 2 * (i % 2))
        return p, (p >= 0) & (p < nz) & (i < steps)

    def forward(i):
        p, ok = plane(i)

        @pl.when(ok & (i > 0))
        def _():
            a_wait(slot(p, c, x))

            @pl.when((p < z) & (z < nz - 1))
            def _():
                a_z(p, True).start()

            @pl.when((p > z) & (z > 0))
            def _():
                a_z(p, False).start()

            a_core(p, x).start()
            for k in range(1, xc):
                a_x(p, k).start()

    def work(i):
        p, ok = plane(i)

        @pl.when(ok)
        def _():
            for k in range(1, xc):
                xb = lax.rem(x + k, xc)
                a_wait(slot(p, c, xb))
                a_core(p, xb).start()
            for xb in range(xc):
                a_wait(slot(p, 1 - c, xb))

            @pl.loop(0, 2)
            def _(j):
                compute(p, (1 - c) * (1 - j) + c * j)

                @pl.when(j == 0)
                def _():
                    r_core(p).start()

            r_core(p).wait_recv()
            for xb in range(xc):
                s = slot(p, c, xb)
                part[s] = (
                    part[s].astype(jnp.float32) + rd[p * xc + xb].astype(jnp.float32)
                ).astype(jnp.bfloat16)
            for k in range(1, xc):
                r_x(p, k).start()

    def settle(i):
        p, ok = plane(i)

        @pl.when(ok & (i >= 0))
        def _():
            s = slot(p, c, x)
            acc = part[s].astype(jnp.float32)
            for k in range(1, xc):
                r_x(p, k).wait_recv()
                acc = acc + rx[p * (xc - 1) + k - 1].astype(jnp.float32)
            part[s] = acc.astype(jnp.bfloat16)

            @pl.when(p != z)
            def _():
                r_z(p).start()

    @pl.loop(0, steps + 1)
    def _(i):
        work(i)
        forward(i + 1)

        @pl.when(i > 0)
        def _():
            settle(i - 1)

    for k in range(1, xc):
        for cp in held_x(k):
            cp.start()
    for cp in held_core(x):
        cp.start()
    for k in range(1, xc):
        xb = lax.rem(x + k, xc)
        ts = xb * CORES + c
        rem(hgu_at(ts), hgu_at(ts), hsend.at[0, k], hrecv.at[0, ts], partner).wait_recv()
        rem(hd_at(ts), hd_at(ts), hsend.at[1, k], hrecv.at[1, ts], partner).wait_recv()
        for cp in held_core(xb):
            cp.start()
    for xb in range(xc):
        ts = xb * CORES + 1 - c
        rem(hgu_at(ts), hgu_at(ts), hsend.at[2, xb], hrecv.at[0, ts], partner).wait_recv()
        rem(hd_at(ts), hd_at(ts), hsend.at[3, xb], hrecv.at[1, ts], partner).wait_recv()
    outs.append(pltpu.make_async_copy(hgu, o_hgu, lsem.at[1]))
    outs.append(pltpu.make_async_copy(hd, o_hd, lsem.at[2]))
    outs[1].start()
    outs[2].start()

    for zs in range(nz):
        @pl.when(zs != z)
        def _():
            rem(rz.at[zs], rz.at[zs], rzsend.at[zs], rzrecv.at[zs], partner).wait_recv()

    acc = part[own].astype(jnp.float32)
    for k in range(1, nz):
        acc = acc + rz[lax.rem(z + k, nz)].astype(jnp.float32)
    mix[...] = acc.astype(jnp.bfloat16)
    outs.append(pltpu.make_async_copy(mix, o_mix, lsem.at[3]))
    outs[3].start()

    @pl.loop(1, n)
    def _(k):
        j = lax.rem(me + k, n)
        for cp in w_send(j):
            cp.wait_send()
        share_send(j).wait_send()
        for cp in w_across(j, g):
            cp.wait_send()

    for send, count in ((sgu_send, nz), (sdn_send, nt)):
        for k in range(count):
            j, cp = send(k)

            @pl.when(j != me)
            def _():
                cp.wait_send()

    for k in range(1, xc):
        for cp in held_x(k):
            cp.wait_send()
    for xb in range(xc):
        for cp in held_core(xb):
            cp.wait_send()

    @pl.loop(0, nz)
    def _(p):
        @pl.when((p <= z) & (z < nz - 1))
        def _():
            a_z(p, True).wait_send()

        @pl.when((p >= z) & (z > 0))
        def _():
            a_z(p, False).wait_send()

        for k in range(1, xc):
            a_x(p, k).wait_send()
            r_x(p, k).wait_send()
        for xb in range(xc):
            a_core(p, xb).wait_send()
        r_core(p).wait_send()

        @pl.when(p != z)
        def _():
            r_z(p).wait_send()

    for cp in outs:
        cp.wait()


def kernel_plan(
    tokens,
    route_ids,
    route_scores,
    norm_gain,
    expert_gate,
    expert_up,
    expert_down,
    shared_gate,
    shared_up,
    shared_down,
):
    nz = lax.axis_size("fs")
    nt = lax.axis_size("tp")
    n = nz * nt
    xc = nt // CORES
    rows, width = tokens.shape
    widened = tokens.astype(jnp.float32)
    normed = (
        widened * lax.rsqrt(jnp.mean(widened * widened, axis=1, keepdims=True) + EPSILON)
    ).astype(jnp.bfloat16)
    weights = route_scale * route_scores / jnp.sum(route_scores, axis=1, keepdims=True)
    named = route_ids.T[None, :, :] == jnp.arange(n, dtype=jnp.int32)[:, None, None]
    shares = jnp.sum(jnp.where(named, weights.T[None], 0.0), axis=1)[:, None, :]
    gu = jnp.stack(
        [
            (norm_gain * jnp.swapaxes(expert_gate, 1, 2)).astype(jnp.bfloat16),
            (norm_gain * jnp.swapaxes(expert_up, 1, 2)).astype(jnp.bfloat16),
        ],
        axis=1,
    )
    dn = expert_down.astype(jnp.bfloat16)
    sgu = jnp.stack(
        [
            (norm_gain * shared_gate.T).astype(jnp.bfloat16),
            (norm_gain * shared_up.T).astype(jnp.bfloat16),
        ],
        axis=0,
    )
    sdn = shared_down.astype(jnp.bfloat16)
    ft, dt = gu.shape[2], gu.shape[3]
    fr, dc = dn.shape[1], dn.shape[2]
    inner = ft * nt
    sd = sgu.shape[1] * nt // n
    bf = jnp.bfloat16
    dma = pltpu.SemaphoreType.DMA
    hbm = pl.BlockSpec(memory_space=pltpu.HBM)
    mixed, wall, hgu, hd = pl.pallas_call(
        functools.partial(handover_kernel, nz, nt),
        out_shape=(
            jax.ShapeDtypeStruct((rows, width), bf),
            jax.ShapeDtypeStruct((3, inner, width), bf),
            jax.ShapeDtypeStruct((2, sgu.shape[1] * nt, dt), bf),
            jax.ShapeDtypeStruct((sdn.shape[0], width), bf),
        ),
        in_specs=[hbm] * 6,
        out_specs=(hbm,) * 4,
        scratch_shapes=[
            pltpu.VMEM((3, inner + sd, width), bf),
            pltpu.VMEM((n, rows, width), bf),
            pltpu.VMEM((n, rows, width), bf),
            pltpu.VMEM((nz * xc, rows, width), bf),
            pltpu.VMEM((nz * (xc - 1), rows, width), bf),
            pltpu.VMEM((nz, rows, width), bf),
            pltpu.VMEM((n, 1, rows), jnp.float32),
            pltpu.VMEM((2, sgu.shape[1] * nt, dt), bf),
            pltpu.VMEM((sdn.shape[0], width), bf),
            pltpu.VMEM((rows, width), bf),
            dma((8,)),
            dma((2, n)),
            dma((2, n)),
            dma((2, n)),
            dma((2, n)),
            dma((n,)),
            dma((n,)),
            dma((2, max(nz, nt))),
            dma((2, max(nz, nt))),
            dma((4, xc)),
            dma((2, nt)),
            dma((2 + xc, n)),
            dma((n,)),
            dma((nz,)),
            dma((nz,)),
            dma((nz, xc)),
            dma((nz, xc)),
            dma((nz,)),
            dma((nz,)),
        ],
        compiler_params=pltpu.CompilerParams(
            collective_id=0, has_side_effects=True, vmem_limit_bytes=60 << 20
        ),
    )(normed, gu, dn, sgu, sdn, shares)
    return (
        mixed,
        wall[0].T[None],
        wall[1].T[None],
        wall[2][None],
        hgu[0].T,
        hgu[1].T,
        hd,
    )


def on_device(*args):
    experts = lax.axis_size("fs") * lax.axis_size("tp")
    picks = args[1].shape[1]
    if experts <= 4 * picks:
        return kernel_plan(*args)
    return dispatch_plan(*args)


def solution(mesh):
    return jax.shard_map(
        on_device,
        mesh=mesh,
        in_specs=(
            P(("grp", "fs", "tp"), None),
            P(("grp", "fs", "tp"), None),
            P(("grp", "fs", "tp"), None),
            P("fs"),
            P(None, "fs", "tp"),
            P(None, "fs", "tp"),
            P(None, "fs", "tp"),
            P("fs", "tp"),
            P("fs", "tp"),
            P("fs", "tp"),
        ),
        out_specs=(
            P(("grp", "fs", "tp"), None),
            P(("grp", "fs", "tp"), None, None),
            P(("grp", "fs", "tp"), None, None),
            P(("grp", "fs", "tp"), None, None),
            P(("grp", "fs"), None),
            P(("grp", "fs"), None),
            P(("grp", "fs"), None),
        ),
        check_vma=False,
    )
```

```python
import functools
import jax
import jax.numpy as jnp
from jax import lax
from jax.experimental import pallas as pl
from jax.experimental.pallas import tpu as pltpu
from jax.sharding import PartitionSpec as P

EPSILON = 1e-06
route_scale = 2.5
CORES = 2
MESH = pl.DeviceIdType.MESH


def expert_rows(row_block, w_gate, w_up, w_down):
    gate_rows = jnp.dot(row_block, w_gate, preferred_element_type=jnp.float32)
    up_rows = jnp.dot(row_block, w_up, preferred_element_type=jnp.float32)
    hidden = (jax.nn.silu(gate_rows) * up_rows).astype(jnp.bfloat16)
    return jnp.dot(hidden, w_down, preferred_element_type=jnp.float32).astype(jnp.bfloat16)


def relayout(arrived, fs_count, tp_count):
    tile_rows = arrived.shape[2]
    tile_cols = arrived.shape[3]
    grid = arrived.reshape(fs_count, tp_count, tile_rows, tile_cols)
    grid = jnp.transpose(grid, (0, 2, 1, 3))
    return grid.reshape(1, fs_count * tile_rows, tp_count * tile_cols)


def dispatch_plan(
    tokens,
    route_ids,
    route_scores,
    norm_gain,
    expert_gate,
    expert_up,
    expert_down,
    shared_gate,
    shared_up,
    shared_down,
):
    fs_count = lax.axis_size("fs")
    tp_count = lax.axis_size("tp")
    experts = fs_count * tp_count
    gain_col = norm_gain[:, None]
    piece_gate = (gain_col[None] * expert_gate).astype(jnp.bfloat16)
    piece_up = (gain_col[None] * expert_up).astype(jnp.bfloat16)
    piece_down = expert_down.astype(jnp.bfloat16)
    moved = (
        lax.all_to_all(piece_gate[:, None], ("fs", "tp"), split_axis=0, concat_axis=1, tiled=True),
        lax.all_to_all(piece_up[:, None], ("fs", "tp"), split_axis=0, concat_axis=1, tiled=True),
        lax.all_to_all(piece_down[:, None], ("fs", "tp"), split_axis=0, concat_axis=1, tiled=True),
    )
    served_gate = relayout(moved[0], fs_count, tp_count)
    served_up = relayout(moved[1], fs_count, tp_count)
    served_down = relayout(moved[2], fs_count, tp_count)
    tile_gate = (gain_col * shared_gate).astype(jnp.bfloat16)
    tile_up = (gain_col * shared_up).astype(jnp.bfloat16)
    tile_down = shared_down.astype(jnp.bfloat16)
    held_gate, held_up, held_down = (
        lax.all_gather(tile_gate, "tp", axis=1, tiled=True),
        lax.all_gather(tile_up, "tp", axis=1, tiled=True),
        lax.all_gather(tile_down, "tp", axis=1, tiled=True),
    )
    rows_dev = tokens.shape[0]
    width = tokens.shape[1]
    picks = route_ids.shape[1]
    capacity = 3 * rows_dev * picks // (2 * experts)
    widened = tokens.astype(jnp.float32)
    normed = (
        widened * lax.rsqrt(jnp.mean(widened * widened, axis=1, keepdims=True) + EPSILON)
    ).astype(jnp.bfloat16)
    weights = route_scale * route_scores / jnp.sum(route_scores, axis=1, keepdims=True)
    flat_ids = route_ids.reshape(-1)
    onehot = (flat_ids[:, None] == jnp.arange(experts, dtype=jnp.int32)[None, :]).astype(jnp.int32)
    earlier = jnp.cumsum(onehot, axis=0) - onehot
    ranks = jnp.sum(earlier * onehot, axis=1)
    target = flat_ids * capacity + ranks
    outbox = (
        jnp.zeros((experts * capacity, width), jnp.bfloat16)
        .at[target]
        .set(jnp.repeat(normed, picks, axis=0))
    )
    arrived = lax.all_to_all(
        outbox.reshape(experts, capacity, width),
        ("fs", "tp"),
        split_axis=0,
        concat_axis=0,
        tiled=True,
    )
    finished = expert_rows(
        arrived.reshape(-1, width), served_gate[0], served_up[0], served_down[0]
    ).reshape(arrived.shape)
    returned = lax.all_to_all(finished, ("fs", "tp"), split_axis=0, concat_axis=0, tiled=True)
    results = returned.reshape(experts * capacity, width)[target]
    routed = jnp.sum(
        results.reshape(rows_dev, picks, width).astype(jnp.float32) * weights[:, :, None], axis=1
    )
    columns = normed
    gate_part = jnp.dot(
        columns,
        lax.all_gather(held_gate, "fs", axis=0, tiled=True),
        preferred_element_type=jnp.float32,
    )
    up_part = jnp.dot(
        columns,
        lax.all_gather(held_up, "fs", axis=0, tiled=True),
        preferred_element_type=jnp.float32,
    )
    shared_hidden = (jax.nn.silu(gate_part) * up_part).astype(jnp.bfloat16)
    columns = shared_hidden
    shared_term = jnp.dot(
        columns,
        lax.all_gather(held_down, "fs", axis=0, tiled=True),
        preferred_element_type=jnp.float32,
    )
    mixed = (routed + shared_term).astype(jnp.bfloat16)
    return (mixed, served_gate, served_up, served_down, held_gate, held_up, held_down)


def handover_kernel(
    nz,
    nt,
    tokens,
    ids,
    scores,
    gain,
    in_gate,
    in_up,
    in_down,
    in_sgate,
    in_sup,
    in_sdown,
    o_mix,
    o_gate,
    o_up,
    o_down,
    o_hgate,
    o_hup,
    o_hd,
    l_tok,
    l_ids,
    l_scores,
    l_gain,
    l_gate,
    l_up,
    l_down,
    l_sgate,
    l_sup,
    l_sdown,
    gu,
    dn,
    sgu,
    sdn,
    shares,
    w,
    tok,
    part,
    rd,
    rx,
    rz,
    ry,
    total,
    share,
    hgu,
    hd,
    flip,
    hflip,
    lsem,
    osem,
    wsend,
    wrecv,
    ysend,
    yrecv,
    shsend,
    shrecv,
    ssend,
    srecv,
    hsend,
    hrecv,
    asend,
    arecv,
    rdsend,
    rdrecv,
    rxsend,
    rxrecv,
    rzsend,
    rzrecv,
    ryrecv,
):
    n = nz * nt
    xc = nt // CORES
    g = lax.axis_index("grp")
    z = lax.axis_index("fs")
    t = lax.axis_index("tp")
    x = t // CORES
    c = t % CORES
    me = z * nt + t
    rows, width = tokens.shape
    ft, dt = in_gate.shape[1], in_gate.shape[2]
    fr, dc = in_down.shape[1], in_down.shape[2]
    st, sr = in_sgate.shape[0], in_sdown.shape[0]
    inner = ft * nt
    sd = w.shape[1] - inner
    half_f, half_r, half_st, half_sr = ft // 2, fr // 2, st // 2, sr // 2

    def dev(zz, tt, gg=None):
        return {"grp": g if gg is None else gg, "fs": zz, "tp": tt}

    def rem(src, dst, ssem, rsem, device):
        return pltpu.make_async_remote_copy(
            src_ref=src,
            dst_ref=dst,
            send_sem=ssem,
            recv_sem=rsem,
            device_id=device,
            device_id_type=MESH,
        )

    def al(v, m):
        return pl.multiple_of(v, m)

    partner = dev(z, x * CORES + 1 - c)
    across = dev(z, t, 1 - g)
    mate = z * nt + x * CORES + 1 - c

    def xdev(k):
        return dev(z, lax.rem(x + k, xc) * CORES + c)

    def slot(p, h, xb):
        return p * nt + h * xc + xb

    own = slot(z, c, x)

    barrier = pltpu.get_barrier_semaphore()

    @pl.loop(1, n)
    def _(k):
        j = lax.rem(me + k, n)
        pl.semaphore_signal(barrier, 1, device_id=dev(j // nt, j % nt), device_id_type=MESH)

    pl.semaphore_signal(barrier, 1, device_id=across, device_id_type=MESH)

    loads = [
        pltpu.make_async_copy(src, dst, lsem.at[i])
        for i, (src, dst) in enumerate(
            (
                (tokens, l_tok),
                (gain, l_gain),
                (in_gate, l_gate),
                (in_up, l_up),
                (in_down, l_down),
                (in_sgate, l_sgate),
                (in_sup, l_sup),
                (in_sdown, l_sdown),
                (ids, l_ids),
                (scores, l_scores),
            )
        )
    ]
    for cp in loads:
        cp.start()
    loads[0].wait()
    band = min(32, rows)

    @pl.loop(0, rows // band)
    def _(r):
        at = pl.ds(al(r * band, band), band)
        wide = l_tok[at, :].astype(jnp.float32)
        mean = jnp.mean(wide * wide, axis=1, keepdims=True)
        tok[own, at, :] = (wide * lax.rsqrt(mean + EPSILON)).astype(jnp.bfloat16)

    for cp in loads[1:]:
        cp.wait()

    @pl.loop(0, n)
    def _(e):
        gu[e, 0] = (l_gain[...] * l_gate[e]).astype(jnp.bfloat16)
        gu[e, 1] = (l_gain[...] * l_up[e]).astype(jnp.bfloat16)
        dn[e] = l_down[e].astype(jnp.bfloat16)

    sgu[0] = (l_gain[...] * l_sgate[...]).astype(jnp.bfloat16)
    sgu[1] = (l_gain[...] * l_sup[...]).astype(jnp.bfloat16)
    sdn[...] = l_sdown[...].astype(jnp.bfloat16)
    sc = l_scores[...]
    mixing = route_scale * sc / jnp.sum(sc, axis=0, keepdims=True)
    for e in range(n):
        shares[e] = jnp.sum(jnp.where(l_ids[...] == e, mixing, 0.0), axis=0, keepdims=True)
    own_gu = (pl.ds(0, 2), pl.ds(al(t * ft, ft), ft), pl.ds(al(z * dt, dt), dt))
    w[own_gu] = gu[me]
    w[2, pl.ds(al(z * fr, fr), fr), pl.ds(al(t * dc, dc), dc)] = dn[me]
    hgu[:, pl.ds(al(t * st, st), st), :] = sgu[...]
    hd[:, pl.ds(al(t * dc, dc), dc)] = sdn[...]
    share[me] = shares[me]

    @pl.when(me // nz == t)
    def _():
        w[pl.ds(0, 2), pl.ds(inner, sd), pl.ds(al(z * dt, dt), dt)] = sgu[
            :, pl.ds(al((me % nz) * sd, sd), sd), :
        ]

    @pl.when(me // nt == z)
    def _():
        w[2, pl.ds(inner, sd), pl.ds(al(t * dc, dc), dc)] = sdn[
            pl.ds(al((me % nt) * sd, sd), sd), :
        ]

    pl.semaphore_wait(barrier, n)

    def gu_at(src, gg):
        zs, ts = src // nt, src % nt
        return w.at[
            pl.ds(0, 2), pl.ds(al(ts * ft + gg * half_f, half_f), half_f), pl.ds(al(zs * dt, dt), dt)
        ]

    def dn_at(src, gg):
        zs, ts = src // nt, src % nt
        return w.at[2, pl.ds(al(zs * fr + gg * half_r, half_r), half_r), pl.ds(al(ts * dc, dc), dc)]

    def w_send(j, gg, ssem, rsem):
        device = dev(j // nt, j % nt)
        return (
            rem(
                gu.at[j, pl.ds(0, 2), pl.ds(al(gg * half_f, half_f), half_f), :],
                gu_at(me, gg),
                ssem.at[0, j],
                rsem.at[0, me],
                device,
            ),
            rem(
                dn.at[j, pl.ds(al(gg * half_r, half_r), half_r), :],
                dn_at(me, gg),
                ssem.at[1, j],
                rsem.at[1, me],
                device,
            ),
        )

    def w_out(j):
        return w_send(j, g, wsend, wrecv)

    def w_mate():
        return w_send(mate, 1 - g, ysend, yrecv)

    def w_across(s, gg):
        return (
            rem(gu_at(s, gg), gu_at(s, gg), ysend.at[0, s], yrecv.at[0, s], across),
            rem(dn_at(s, gg), dn_at(s, gg), ysend.at[1, s], yrecv.at[1, s], across),
        )

    def w_plane_send(p):
        @pl.loop(0, nt)
        def _(tt):
            for cp in w_out(p * nt + tt):
                cp.start()

    def w_plane_across(p):
        @pl.loop(0, nt)
        def _(tt):
            s = p * nt + tt
            for i, at in ((0, gu_at), (1, dn_at)):
                rem(at(s, g), at(s, g), ysend.at[i, s], wrecv.at[i, s], across).wait_recv()
            for cp in w_across(s, g):
                cp.start()

    def share_send(j):
        return rem(shares.at[j], share.at[me], shsend.at[j], shrecv.at[me], dev(j // nt, j % nt))

    def sgu_at(zs):
        return w.at[pl.ds(0, 2), pl.ds(inner, sd), pl.ds(al(zs * dt, dt), dt)]

    def sdn_at(ts):
        return w.at[2, pl.ds(inner, sd), pl.ds(al(ts * dc, dc), dc)]

    def sgu_send(k):
        j = t * nz + k
        return j, rem(
            sgu.at[pl.ds(0, 2), pl.ds(k * sd, sd), :],
            sgu_at(z),
            ssend.at[0, k],
            srecv.at[0, z],
            dev(j // nt, j % nt),
        )

    def sdn_send(k):
        j = z * nt + k
        return j, rem(
            sdn.at[pl.ds(k * sd, sd), :],
            sdn_at(t),
            ssend.at[1, k],
            srecv.at[1, t],
            dev(j // nt, j % nt),
        )

    def hgu_half(ts, gg):
        return hgu.at[pl.ds(0, 2), pl.ds(al(ts * st + gg * half_st, half_st), half_st), :]

    def hd_half(ts, gg):
        return hd.at[pl.ds(al(gg * half_sr, half_sr), half_sr), pl.ds(al(ts * dc, dc), dc)]

    def hgu_at(ts):
        return hgu.at[pl.ds(0, 2), pl.ds(al(ts * st, st), st), :]

    def hd_at(ts):
        return hd.at[:, pl.ds(al(ts * dc, dc), dc)]

    def held_x(k):
        return (
            rem(
                sgu.at[pl.ds(0, 2), pl.ds(al(g * half_st, half_st), half_st), :],
                hgu_half(t, g),
                hsend.at[0, t],
                hrecv.at[0, t],
                xdev(k),
            ),
            rem(
                sdn.at[pl.ds(al(g * half_sr, half_sr), half_sr), :],
                hd_half(t, g),
                hsend.at[1, t],
                hrecv.at[1, t],
                xdev(k),
            ),
        )

    def held_x_in(ts):
        return (
            rem(hgu_half(ts, g), hgu_half(ts, g), hsend.at[0, ts], hrecv.at[0, ts], across),
            rem(hd_half(ts, g), hd_half(ts, g), hsend.at[1, ts], hrecv.at[1, ts], across),
        )

    def held_across(ts, gg):
        return (
            rem(hgu_half(ts, gg), hgu_half(ts, gg), hsend.at[2, ts], hrecv.at[2, ts], across),
            rem(hd_half(ts, gg), hd_half(ts, gg), hsend.at[3, ts], hrecv.at[3, ts], across),
        )

    def held_core(ts):
        return (
            rem(hgu_at(ts), hgu_at(ts), hsend.at[4, ts], hrecv.at[4, ts], partner),
            rem(hd_at(ts), hd_at(ts), hsend.at[5, ts], hrecv.at[5, ts], partner),
        )

    def a_z(p, up):
        s = slot(p, c, x)
        return rem(
            tok.at[s],
            tok.at[s],
            asend.at[0 if up else 1, s],
            arecv.at[s],
            dev(z + 1 if up else z - 1, t),
        )

    def a_x(p, k):
        s = slot(p, c, x)
        return rem(tok.at[s], tok.at[s], asend.at[2 + k, s], arecv.at[s], xdev(k))

    def a_core(p, xb):
        s = slot(p, c, xb)
        return rem(tok.at[s], tok.at[s], asend.at[2, s], arecv.at[s], partner)

    def a_wait(s):
        rem(tok.at[s], tok.at[s], asend.at[2, s], arecv.at[s], partner).wait_recv()

    def a_cross(p):
        for k in range(1, xc):
            xb = lax.rem(x + k, xc)
            a_wait(slot(p, c, xb))
            a_core(p, xb).start()

    def r_core(p):
        return rem(
            part.at[pl.ds(slot(p, 1 - c, 0), xc)],
            rd.at[pl.ds(p * xc, xc)],
            rdsend.at[p],
            rdrecv.at[p],
            partner,
        )

    def r_x(p, k):
        xb = lax.rem(x + k, xc)
        return rem(
            part.at[slot(p, c, xb)],
            rx.at[p * (xc - 1) + k - 1],
            rxsend.at[p, k - 1],
            rxrecv.at[p, k - 1],
            xdev(k),
        )

    def r_z(p):
        return rem(part.at[slot(p, c, x)], rz.at[z], rzsend.at[p], rzrecv.at[z], dev(p, t))

    near = jnp.where(z == 0, 1, nz - 2)

    def r_relay(p):
        return rem(part.at[slot(p, c, x)], ry.at[p], rzsend.at[p], ryrecv.at[p], dev(near, t))

    def relayed(p):
        return ((z == 1) & (p > 1)) | ((z == nz - 2) & (p < nz - 2))

    @pl.loop(1, nt)
    def _(k):
        for cp in w_out(z * nt + lax.rem(t + k, nt)):
            cp.start()

    for cp in w_mate():
        cp.start()

    @pl.when(z < nz - 1)
    def _():
        a_z(z, True).start()

    @pl.when(z > 0)
    def _():
        a_z(z, False).start()

    a_core(z, x).start()
    for k in range(1, xc):
        a_x(z, k).start()

    @pl.loop(1, n)
    def _(k):
        share_send(lax.rem(me + k, n)).start()

    def send_when(j, cp):
        @pl.when(j != me)
        def _():
            cp.start()

    last = jnp.where(2 * z < nz, nz - 1 - z, z)

    edge = (z == 0) | (z == nz - 1)

    @pl.loop(0, nz + 1)
    def _(d):
        late = edge & (d == nz - 1)

        @pl.when((d > 0) & (z - d >= 0) & ~late)
        def _():
            p = z - d
            a_wait(slot(p, c, x))

            @pl.when(z < nz - 1)
            def _():
                a_z(p, True).start()

            for k in range(1, xc):
                a_x(p, k).start()
            a_core(p, x).start()

        @pl.when((d > 0) & (z + d < nz) & ~late)
        def _():
            p = z + d
            a_wait(slot(p, c, x))

            @pl.when(z > 0)
            def _():
                a_z(p, False).start()

            for k in range(1, xc):
                a_x(p, k).start()
            a_core(p, x).start()

        @pl.when(d == nz - 1)
        def _():
            for send, count in ((sgu_send, nz), (sdn_send, nt)):
                for k in range(count):
                    send_when(*send(k))

            for k in range(1, xc):
                for cp in held_x(k):
                    cp.start()

        @pl.when(d < nz)
        def _():
            stop = jnp.where(edge | (d < last), d, nz - 1)

            @pl.loop(d, stop + 1)
            def _(q):
                @pl.when((q > z) & (edge | (d <= last)))
                def _():
                    w_plane_send(q)

                @pl.when((nz - 1 - q < z) & (edge | (d <= last)))
                def _():
                    w_plane_send(nz - 1 - q)

        @pl.when(d == 1)
        def _():
            @pl.loop(1, nt)
            def _(k):
                s = z * nt + lax.rem(t + k, nt)
                for i, at in ((0, gu_at), (1, dn_at)):
                    rem(at(s, g), at(s, g), ysend.at[i, s], wrecv.at[i, s], across).wait_recv()

                @pl.when(s != mate)
                def _():
                    for cp in w_across(s, g):
                        cp.start()

        @pl.when(late)
        def _():
            p = nz - 1 - z
            w_plane_across(p)
            a_wait(slot(p, c, x))
            for k in range(1, xc):
                a_x(p, k).start()
            a_core(p, x).start()

        @pl.when((d == z + 1) & (z < nz - 1))
        def _():
            @pl.loop(0, z)
            def _(p):
                w_plane_across(p)

        @pl.when((d == nz - z) & (z > 0))
        def _():
            @pl.loop(z + 1, nz)
            def _(k):
                w_plane_across(nz + z - k)

        @pl.when(edge & (d == nz))
        def _():
            @pl.loop(1, nz - 1)
            def _(k):
                w_plane_across(jnp.where(z == 0, nz - 1 - k, k))

    @pl.loop(0, nz)
    def _(k):
        a_cross(lax.rem(z + k, nz))

    for k in range(1, xc):
        ts = lax.rem(x + k, xc) * CORES + c
        for cp in held_x_in(ts):
            cp.wait_recv()
        for cp in held_across(ts, g):
            cp.start()

    @pl.loop(1, n)
    def _(k):
        s = lax.rem(me + n - k, n)
        for cp in w_across(s, 1 - g):
            cp.wait_recv()
        rem(shares.at[s], share.at[s], shsend.at[s], shrecv.at[s], across).wait_recv()

    for k in range(nz):

        @pl.when(k * nt + me // nz != me)
        def _():
            rem(sgu_at(k), sgu_at(k), ssend.at[0, k], srecv.at[0, k], across).wait_recv()

    for k in range(nt):

        @pl.when((me // nt) * nt + k != me)
        def _():
            rem(sdn_at(k), sdn_at(k), ssend.at[1, k], srecv.at[1, k], across).wait_recv()

    out_down = pltpu.make_async_copy(w.at[2, pl.ds(0, inner), :], o_down, osem.at[0])
    out_down.start()
    nt_dims = (((1,), (1,)), ((), ()))

    def compute(p, h):
        first = slot(p, h, 0)
        xs = tok[pl.ds(first, xc)].reshape(xc * rows, width)
        gate = lax.dot_general(xs, w[0], nt_dims, preferred_element_type=jnp.float32)
        up = lax.dot_general(xs, w[1], nt_dims, preferred_element_type=jnp.float32)
        hidden = gate / (1.0 + jnp.exp(-gate)) * up
        scale = jnp.concatenate(
            [
                jnp.transpose(jnp.broadcast_to(share[p * nt + xb * CORES + h], (rows, rows)))
                for xb in range(xc)
            ],
            axis=0,
        )[:, :1]
        col = lax.broadcasted_iota(jnp.int32, hidden.shape, 1)
        hidden = jnp.where(col < inner, hidden * scale, hidden).astype(jnp.bfloat16)
        step = min(512, width)
        for lo in range(0, width, step):
            res = jnp.dot(hidden, w[2, :, lo : lo + step], preferred_element_type=jnp.float32)
            part[pl.ds(first, xc), :, lo : lo + step] = res.astype(jnp.bfloat16).reshape(
                xc, rows, step
            )

    def work(p):
        for xb in range(xc):
            a_wait(slot(p, 1 - c, xb))

        @pl.loop(0, 2)
        def _(j):
            compute(p, (1 - c) * (1 - j) + c * j)

            @pl.when(j == 0)
            def _():
                r_core(p).start()

        r_core(p).wait_recv()
        for k in range(1, xc):
            xb = lax.rem(x + k, xc)
            s = slot(p, c, xb)
            part[s] = (part[s].astype(jnp.float32) + rd[p * xc + xb].astype(jnp.float32)).astype(
                jnp.bfloat16
            )
            r_x(p, k).start()

    def settle(p):
        s = slot(p, c, x)
        acc = part[s].astype(jnp.float32) + rd[p * xc + x].astype(jnp.float32)
        for k in range(1, xc):
            r_x(p, k).wait_recv()
            acc = acc + rx[p * (xc - 1) + k - 1].astype(jnp.float32)
        part[s] = acc.astype(jnp.bfloat16)

        @pl.when(relayed(p))
        def _():
            r_relay(p).wait_recv()
            part[s] = (acc + ry[p].astype(jnp.float32)).astype(jnp.bfloat16)

    low = 2 * z < nz

    def order(i):
        q = jnp.where(edge, i, jnp.where(i == 0, 0, nz - i))
        inside = jnp.where(q == 0, jnp.where(low, 0, nz - 1), jnp.where(low, q, nz - 1 - q))
        ends = jnp.where(low, nz - 1 - i, i)
        return jnp.where(i == nz - 1, z, jnp.where(edge, ends, inside))

    @pl.loop(0, nz)
    def _(i):
        work(order(i))

        @pl.when(i == 0)
        def _():
            for i2 in range(2):
                for lo in range(0, width, 256):
                    flip[i2, lo : lo + 256, :] = jnp.transpose(w[i2, :inner, lo : lo + 256])
            for i2, o_w in enumerate((o_gate, o_up)):
                pltpu.make_async_copy(flip.at[i2], o_w, osem.at[1 + i2]).start()

        @pl.when(i > 0)
        def _():
            p = order(i - 1)
            settle(p)

            @pl.when(edge & (p != near))
            def _():
                r_relay(p).start()

            @pl.when(~edge | (p == near))
            def _():
                r_z(p).start()

    for k in range(1, xc):
        ts = lax.rem(x + k, xc) * CORES + c
        for cp in held_across(ts, 1 - g):
            cp.wait_recv()
    for xb in range(xc):
        for cp in held_core(xb * CORES + c):
            cp.start()
    for xb in range(xc):
        for cp in held_core(xb * CORES + 1 - c):
            cp.wait_recv()
    for i in range(2):
        hflip[i] = jnp.transpose(hgu[i])
    out_held = [
        pltpu.make_async_copy(hflip.at[0], o_hgate, osem.at[3]),
        pltpu.make_async_copy(hflip.at[1], o_hup, osem.at[4]),
        pltpu.make_async_copy(hd, o_hd, osem.at[6]),
    ]
    for cp in out_held:
        cp.start()

    settle(z)
    total[...] = part[own].astype(jnp.float32)
    for k in range(1, nz):
        zs = lax.rem(z + k, nz)

        @pl.when(((zs > 0) & (zs < nz - 1)) | (zs == z + 1) | (zs == z - 1))
        def _():
            rem(rz.at[zs], rz.at[zs], rzsend.at[zs], rzrecv.at[zs], partner).wait_recv()
            total[...] += rz[zs].astype(jnp.float32)

    l_tok[...] = total[...].astype(jnp.bfloat16)
    out_mix = pltpu.make_async_copy(l_tok, o_mix, osem.at[5])
    out_mix.start()

    @pl.loop(1, n)
    def _(k):
        j = lax.rem(me + k, n)
        for cp in w_out(j):
            cp.wait_send()
        share_send(j).wait_send()
        for cp in w_across(j, g):
            cp.wait_send()

    for send, count in ((sgu_send, nz), (sdn_send, nt)):
        for k in range(count):
            j, cp = send(k)

            @pl.when(j != me)
            def _():
                cp.wait_send()

    for k in range(1, xc):
        for cp in held_x(k):
            cp.wait_send()
        for cp in held_across(lax.rem(x + k, xc) * CORES + c, g):
            cp.wait_send()
    for xb in range(xc):
        for cp in held_core(xb * CORES + c):
            cp.wait_send()

    @pl.loop(0, nz)
    def _(p):
        @pl.when((p <= z) & (z < nz - 1))
        def _():
            a_z(p, True).wait_send()

        @pl.when((p >= z) & (z > 0))
        def _():
            a_z(p, False).wait_send()

        for k in range(1, xc):
            a_x(p, k).wait_send()
            r_x(p, k).wait_send()
        for xb in range(xc):
            a_core(p, xb).wait_send()
        r_core(p).wait_send()

        @pl.when(p != z)
        def _():
            r_z(p).wait_send()

    out_down.wait()
    for i, o_w in enumerate((o_gate, o_up)):
        pltpu.make_async_copy(flip.at[i], o_w, osem.at[1 + i]).wait()
    for cp in out_held:
        cp.wait()
    out_mix.wait()


def kernel_plan(
    tokens,
    route_ids,
    route_scores,
    norm_gain,
    expert_gate,
    expert_up,
    expert_down,
    shared_gate,
    shared_up,
    shared_down,
):
    nz = lax.axis_size("fs")
    nt = lax.axis_size("tp")
    n = nz * nt
    xc = nt // CORES
    rows, width = tokens.shape
    picks = route_ids.shape[1]
    dt, ft = expert_gate.shape[1:]
    fr, dc = expert_down.shape[1:]
    st, sr = shared_gate.shape[1], shared_down.shape[0]
    inner = ft * nt
    sd = st * nt // n
    bf, f4 = jnp.bfloat16, jnp.float32
    dma = pltpu.SemaphoreType.DMA
    hbm = pl.BlockSpec(memory_space=pltpu.HBM)
    outs = (
        (rows, width),
        (width, inner),
        (width, inner),
        (inner, width),
        (dt, st * nt),
        (dt, st * nt),
        (sr, width),
    )
    mixed, gate, up, down, hgate, hup, hd = pl.pallas_call(
        functools.partial(handover_kernel, nz, nt),
        out_shape=tuple(jax.ShapeDtypeStruct(s, bf) for s in outs),
        in_specs=[hbm] * 10,
        out_specs=(hbm,) * len(outs),
        scratch_shapes=[
            pltpu.VMEM((rows, width), bf),
            pltpu.VMEM((picks, rows), jnp.int32),
            pltpu.VMEM((picks, rows), f4),
            pltpu.VMEM((1, dt), f4),
            pltpu.VMEM((n, ft, dt), f4),
            pltpu.VMEM((n, ft, dt), f4),
            pltpu.VMEM((n, fr, dc), f4),
            pltpu.VMEM((st, dt), f4),
            pltpu.VMEM((st, dt), f4),
            pltpu.VMEM((sr, dc), f4),
            pltpu.VMEM((n, 2, ft, dt), bf),
            pltpu.VMEM((n, fr, dc), bf),
            pltpu.VMEM((2, st, dt), bf),
            pltpu.VMEM((sr, dc), bf),
            pltpu.VMEM((n, 1, rows), f4),
            pltpu.VMEM((3, inner + sd, width), bf),
            pltpu.VMEM((n, rows, width), bf),
            pltpu.VMEM((n, rows, width), bf),
            pltpu.VMEM((nz * xc, rows, width), bf),
            pltpu.VMEM((nz * (xc - 1), rows, width), bf),
            pltpu.VMEM((nz, rows, width), bf),
            pltpu.VMEM((nz, rows, width), bf),
            pltpu.VMEM((rows, width), f4),
            pltpu.VMEM((n, 1, rows), f4),
            pltpu.VMEM((2, st * nt, dt), bf),
            pltpu.VMEM((sr, width), bf),
            pltpu.VMEM((2, width, inner), bf),
            pltpu.VMEM((2, dt, st * nt), bf),
            dma((10,)),
            dma((7,)),
            dma((2, n)),
            dma((2, n)),
            dma((2, n)),
            dma((2, n)),
            dma((n,)),
            dma((n,)),
            dma((2, max(nz, nt))),
            dma((2, max(nz, nt))),
            dma((6, nt)),
            dma((6, nt)),
            dma((2 + xc, n)),
            dma((n,)),
            dma((nz,)),
            dma((nz,)),
            dma((nz, xc)),
            dma((nz, xc)),
            dma((nz,)),
            dma((nz,)),
            dma((nz,)),
        ],
        compiler_params=pltpu.CompilerParams(
            collective_id=0, has_side_effects=True, vmem_limit_bytes=60 << 20
        ),
    )(
        tokens,
        route_ids.T,
        route_scores.T,
        norm_gain[None],
        jnp.swapaxes(expert_gate, 1, 2),
        jnp.swapaxes(expert_up, 1, 2),
        expert_down,
        shared_gate.T,
        shared_up.T,
        shared_down,
    )
    return mixed, gate[None], up[None], down[None], hgate, hup, hd


def on_device(*args):
    experts = lax.axis_size("fs") * lax.axis_size("tp")
    picks = args[1].shape[1]
    if experts <= 4 * picks:
        return kernel_plan(*args)
    return dispatch_plan(*args)


def solution(mesh):
    return jax.shard_map(
        on_device,
        mesh=mesh,
        in_specs=(
            P(("grp", "fs", "tp"), None),
            P(("grp", "fs", "tp"), None),
            P(("grp", "fs", "tp"), None),
            P("fs"),
            P(None, "fs", "tp"),
            P(None, "fs", "tp"),
            P(None, "fs", "tp"),
            P("fs", "tp"),
            P("fs", "tp"),
            P("fs", "tp"),
        ),
        out_specs=(
            P(("grp", "fs", "tp"), None),
            P(("grp", "fs", "tp"), None, None),
            P(("grp", "fs", "tp"), None, None),
            P(("grp", "fs", "tp"), None, None),
            P(("grp", "fs"), None),
            P(("grp", "fs"), None),
            P(("grp", "fs"), None),
        ),
        check_vma=False,
    )
```

```python
import functools
import jax
import jax.numpy as jnp
from jax import lax
from jax.experimental import pallas as pl
from jax.experimental.pallas import tpu as pltpu
from jax.sharding import PartitionSpec as P

EPSILON = 1e-06
route_scale = 2.5
CORES = 2
PIECES = 2
MESH = pl.DeviceIdType.MESH


def expert_rows(row_block, w_gate, w_up, w_down):
    gate_rows = jnp.dot(row_block, w_gate, preferred_element_type=jnp.float32)
    up_rows = jnp.dot(row_block, w_up, preferred_element_type=jnp.float32)
    hidden = (jax.nn.silu(gate_rows) * up_rows).astype(jnp.bfloat16)
    return jnp.dot(hidden, w_down, preferred_element_type=jnp.float32).astype(jnp.bfloat16)


def relayout(arrived, fs_count, tp_count):
    tile_rows = arrived.shape[2]
    tile_cols = arrived.shape[3]
    grid = arrived.reshape(fs_count, tp_count, tile_rows, tile_cols)
    grid = jnp.transpose(grid, (0, 2, 1, 3))
    return grid.reshape(1, fs_count * tile_rows, tp_count * tile_cols)


def dispatch_plan(
    tokens,
    route_ids,
    route_scores,
    norm_gain,
    expert_gate,
    expert_up,
    expert_down,
    shared_gate,
    shared_up,
    shared_down,
):
    fs_count = lax.axis_size("fs")
    tp_count = lax.axis_size("tp")
    experts = fs_count * tp_count
    gain_col = norm_gain[:, None]
    piece_gate = (gain_col[None] * expert_gate).astype(jnp.bfloat16)
    piece_up = (gain_col[None] * expert_up).astype(jnp.bfloat16)
    piece_down = expert_down.astype(jnp.bfloat16)
    moved = (
        lax.all_to_all(piece_gate[:, None], ("fs", "tp"), split_axis=0, concat_axis=1, tiled=True),
        lax.all_to_all(piece_up[:, None], ("fs", "tp"), split_axis=0, concat_axis=1, tiled=True),
        lax.all_to_all(piece_down[:, None], ("fs", "tp"), split_axis=0, concat_axis=1, tiled=True),
    )
    served_gate = relayout(moved[0], fs_count, tp_count)
    served_up = relayout(moved[1], fs_count, tp_count)
    served_down = relayout(moved[2], fs_count, tp_count)
    tile_gate = (gain_col * shared_gate).astype(jnp.bfloat16)
    tile_up = (gain_col * shared_up).astype(jnp.bfloat16)
    tile_down = shared_down.astype(jnp.bfloat16)
    held_gate, held_up, held_down = (
        lax.all_gather(tile_gate, "tp", axis=1, tiled=True),
        lax.all_gather(tile_up, "tp", axis=1, tiled=True),
        lax.all_gather(tile_down, "tp", axis=1, tiled=True),
    )
    rows_dev = tokens.shape[0]
    width = tokens.shape[1]
    picks = route_ids.shape[1]
    capacity = 3 * rows_dev * picks // (2 * experts)
    widened = tokens.astype(jnp.float32)
    normed = (
        widened * lax.rsqrt(jnp.mean(widened * widened, axis=1, keepdims=True) + EPSILON)
    ).astype(jnp.bfloat16)
    weights = route_scale * route_scores / jnp.sum(route_scores, axis=1, keepdims=True)
    flat_ids = route_ids.reshape(-1)
    onehot = (flat_ids[:, None] == jnp.arange(experts, dtype=jnp.int32)[None, :]).astype(jnp.int32)
    earlier = jnp.cumsum(onehot, axis=0) - onehot
    ranks = jnp.sum(earlier * onehot, axis=1)
    target = flat_ids * capacity + ranks
    outbox = (
        jnp.zeros((experts * capacity, width), jnp.bfloat16)
        .at[target]
        .set(jnp.repeat(normed, picks, axis=0))
    )
    arrived = lax.all_to_all(
        outbox.reshape(experts, capacity, width),
        ("fs", "tp"),
        split_axis=0,
        concat_axis=0,
        tiled=True,
    )
    finished = expert_rows(
        arrived.reshape(-1, width), served_gate[0], served_up[0], served_down[0]
    ).reshape(arrived.shape)
    returned = lax.all_to_all(finished, ("fs", "tp"), split_axis=0, concat_axis=0, tiled=True)
    results = returned.reshape(experts * capacity, width)[target]
    routed = jnp.sum(
        results.reshape(rows_dev, picks, width).astype(jnp.float32) * weights[:, :, None], axis=1
    )
    columns = normed
    gate_part = jnp.dot(
        columns,
        lax.all_gather(held_gate, "fs", axis=0, tiled=True),
        preferred_element_type=jnp.float32,
    )
    up_part = jnp.dot(
        columns,
        lax.all_gather(held_up, "fs", axis=0, tiled=True),
        preferred_element_type=jnp.float32,
    )
    shared_hidden = (jax.nn.silu(gate_part) * up_part).astype(jnp.bfloat16)
    columns = shared_hidden
    shared_term = jnp.dot(
        columns,
        lax.all_gather(held_down, "fs", axis=0, tiled=True),
        preferred_element_type=jnp.float32,
    )
    mixed = (routed + shared_term).astype(jnp.bfloat16)
    return (mixed, served_gate, served_up, served_down, held_gate, held_up, held_down)


def plane_orders(nz):
    far = [p for p in [nz - 2, nz - 1] + list(range(nz - 3, 0, -1)) if p > 0]
    orders = []
    for z in range(nz):
        low = 2 * z < nz
        q = z if low else nz - 1 - z
        planes = [p for p in [0] + far if p != q] + [q]
        orders.append(planes if low else [nz - 1 - p for p in planes])
    return orders


def handover_kernel(
    nz,
    nt,
    tokens,
    ids,
    scores,
    gain,
    in_gate,
    in_up,
    in_down,
    in_sgate,
    in_sup,
    in_sdown,
    o_mix,
    o_gate,
    o_up,
    o_down,
    o_hgate,
    o_hup,
    o_hd,
    l_tok,
    l_ids,
    l_scores,
    l_gain,
    l_gate,
    l_up,
    l_down,
    l_sgate,
    l_sup,
    l_sdown,
    gu,
    dn,
    sgu,
    sdn,
    shares,
    w,
    tok,
    part,
    rd,
    rx,
    rz,
    ry,
    total,
    share,
    hgu,
    hd,
    flip,
    hflip,
    lsem,
    osem,
    wsend,
    wrecv,
    ysend,
    yrecv,
    shsend,
    shrecv,
    ssend,
    srecv,
    hsend,
    hrecv,
    azsend,
    axsend,
    acsend,
    arecv,
    rdsend,
    rdrecv,
    rxsend,
    rxrecv,
    rzsend,
    rzrecv,
    ryrecv,
):
    n = nz * nt
    xc = nt // CORES
    g = lax.axis_index("grp")
    z = lax.axis_index("fs")
    t = lax.axis_index("tp")
    x = t // CORES
    c = t % CORES
    me = z * nt + t
    rows, width = tokens.shape
    ft, dt = in_gate.shape[1], in_gate.shape[2]
    fr, dc = in_down.shape[1], in_down.shape[2]
    st, sr = in_sgate.shape[0], in_sdown.shape[0]
    inner = ft * nt
    sd = w.shape[1] - inner
    half_f, half_r, half_st, half_sr = ft // 2, fr // 2, st // 2, sr // 2

    def dev(zz, tt, gg=None):
        return {"grp": g if gg is None else gg, "fs": zz, "tp": tt}

    def rem(src, dst, ssem, rsem, device):
        return pltpu.make_async_remote_copy(
            src_ref=src,
            dst_ref=dst,
            send_sem=ssem,
            recv_sem=rsem,
            device_id=device,
            device_id_type=MESH,
        )

    def al(v, m):
        return pl.multiple_of(v, m)

    partner = dev(z, x * CORES + 1 - c)
    across = dev(z, t, 1 - g)
    mate = z * nt + x * CORES + 1 - c

    def xdev(k):
        return dev(z, lax.rem(x + k, xc) * CORES + c)

    def slot(p, h, xb):
        return p * nt + h * xc + xb

    own = slot(z, c, x)

    barrier = pltpu.get_barrier_semaphore()

    @pl.loop(1, n)
    def _(k):
        j = lax.rem(me + k, n)
        pl.semaphore_signal(barrier, 1, device_id=dev(j // nt, j % nt), device_id_type=MESH)

    pl.semaphore_signal(barrier, 1, device_id=across, device_id_type=MESH)

    loads = [
        pltpu.make_async_copy(src, dst, lsem.at[i])
        for i, (src, dst) in enumerate(
            (
                (tokens, l_tok),
                (gain, l_gain),
                (in_gate, l_gate),
                (in_up, l_up),
                (in_down, l_down),
                (in_sgate, l_sgate),
                (in_sup, l_sup),
                (in_sdown, l_sdown),
                (ids, l_ids),
                (scores, l_scores),
            )
        )
    ]
    for cp in loads:
        cp.start()
    loads[0].wait()
    band = min(32, rows)

    @pl.loop(0, rows // band)
    def _(r):
        at = pl.ds(al(r * band, band), band)
        wide = l_tok[at, :].astype(jnp.float32)
        mean = jnp.mean(wide * wide, axis=1, keepdims=True)
        tok[own, at, :] = (wide * lax.rsqrt(mean + EPSILON)).astype(jnp.bfloat16)

    for cp in loads[1:]:
        cp.wait()

    @pl.loop(0, n)
    def _(e):
        gu[e, 0] = (l_gain[...] * l_gate[e]).astype(jnp.bfloat16)
        gu[e, 1] = (l_gain[...] * l_up[e]).astype(jnp.bfloat16)
        dn[e] = l_down[e].astype(jnp.bfloat16)

    sgu[0] = (l_gain[...] * l_sgate[...]).astype(jnp.bfloat16)
    sgu[1] = (l_gain[...] * l_sup[...]).astype(jnp.bfloat16)
    sdn[...] = l_sdown[...].astype(jnp.bfloat16)
    sc = l_scores[...]
    mixing = route_scale * sc / jnp.sum(sc, axis=0, keepdims=True)
    for e in range(n):
        shares[e] = jnp.sum(jnp.where(l_ids[...] == e, mixing, 0.0), axis=0, keepdims=True)
    own_gu = (pl.ds(0, 2), pl.ds(al(t * ft, ft), ft), pl.ds(al(z * dt, dt), dt))
    w[own_gu] = gu[me]
    w[2, pl.ds(al(z * fr, fr), fr), pl.ds(al(t * dc, dc), dc)] = dn[me]
    hgu[:, pl.ds(al(t * st, st), st), :] = sgu[...]
    hd[:, pl.ds(al(t * dc, dc), dc)] = sdn[...]
    share[me] = shares[me]

    @pl.when(me // nz == t)
    def _():
        w[pl.ds(0, 2), pl.ds(inner, sd), pl.ds(al(z * dt, dt), dt)] = sgu[
            :, pl.ds(al((me % nz) * sd, sd), sd), :
        ]

    @pl.when(me // nt == z)
    def _():
        w[2, pl.ds(inner, sd), pl.ds(al(t * dc, dc), dc)] = sdn[
            pl.ds(al((me % nt) * sd, sd), sd), :
        ]

    pl.semaphore_wait(barrier, n)

    def gu_at(src, gg):
        zs, ts = src // nt, src % nt
        return w.at[
            pl.ds(0, 2), pl.ds(al(ts * ft + gg * half_f, half_f), half_f), pl.ds(al(zs * dt, dt), dt)
        ]

    def dn_at(src, gg):
        zs, ts = src // nt, src % nt
        return w.at[2, pl.ds(al(zs * fr + gg * half_r, half_r), half_r), pl.ds(al(ts * dc, dc), dc)]

    def w_send(j, gg, ssem, rsem):
        device = dev(j // nt, j % nt)
        return (
            rem(
                gu.at[j, pl.ds(0, 2), pl.ds(al(gg * half_f, half_f), half_f), :],
                gu_at(me, gg),
                ssem.at[0],
                rsem.at[0, me],
                device,
            ),
            rem(
                dn.at[j, pl.ds(al(gg * half_r, half_r), half_r), :],
                dn_at(me, gg),
                ssem.at[1],
                rsem.at[1, me],
                device,
            ),
        )

    def w_out(j):
        return w_send(j, g, wsend, wrecv)

    def w_mate():
        return w_send(mate, 1 - g, wsend, yrecv)

    def w_across(s, gg):
        return (
            rem(gu_at(s, gg), gu_at(s, gg), ysend.at[0], yrecv.at[0, s], across),
            rem(dn_at(s, gg), dn_at(s, gg), ysend.at[1], yrecv.at[1, s], across),
        )

    def w_plane_send(p):
        @pl.loop(0, nt)
        def _(k):
            for cp in w_out(p * nt + lax.rem(t + k, nt)):
                cp.start()

    def w_planes_across(count, plane):
        @pl.loop(0, nt)
        def _(k):
            @pl.loop(0, count)
            def _(i):
                s = plane(i) * nt + lax.rem(t + nt - k, nt)
                for m, at in ((0, gu_at), (1, dn_at)):
                    rem(at(s, g), at(s, g), ysend.at[0], wrecv.at[m, s], across).wait_recv()
                for cp in w_across(s, g):
                    cp.start()

    def share_send(j):
        return rem(shares.at[j], share.at[me], shsend.at[j], shrecv.at[me], dev(j // nt, j % nt))

    def sgu_at(zs):
        return w.at[pl.ds(0, 2), pl.ds(inner, sd), pl.ds(al(zs * dt, dt), dt)]

    def sdn_at(ts):
        return w.at[2, pl.ds(inner, sd), pl.ds(al(ts * dc, dc), dc)]

    def sgu_send(k):
        j = t * nz + k
        return j, rem(
            sgu.at[pl.ds(0, 2), pl.ds(k * sd, sd), :],
            sgu_at(z),
            ssend.at[0, k],
            srecv.at[0, z],
            dev(j // nt, j % nt),
        )

    def sdn_send(k):
        j = z * nt + k
        return j, rem(
            sdn.at[pl.ds(k * sd, sd), :],
            sdn_at(t),
            ssend.at[1, k],
            srecv.at[1, t],
            dev(j // nt, j % nt),
        )

    def hgu_half(ts, gg):
        return hgu.at[pl.ds(0, 2), pl.ds(al(ts * st + gg * half_st, half_st), half_st), :]

    def hd_half(ts, gg):
        return hd.at[pl.ds(al(gg * half_sr, half_sr), half_sr), pl.ds(al(ts * dc, dc), dc)]

    def hgu_at(ts):
        return hgu.at[pl.ds(0, 2), pl.ds(al(ts * st, st), st), :]

    def hd_at(ts):
        return hd.at[:, pl.ds(al(ts * dc, dc), dc)]

    def held_x(k):
        return (
            rem(
                sgu.at[pl.ds(0, 2), pl.ds(al(g * half_st, half_st), half_st), :],
                hgu_half(t, g),
                hsend.at[0, x],
                hrecv.at[0, x],
                xdev(k),
            ),
            rem(
                sdn.at[pl.ds(al(g * half_sr, half_sr), half_sr), :],
                hd_half(t, g),
                hsend.at[1, x],
                hrecv.at[1, x],
                xdev(k),
            ),
        )

    def held_x_in(ts):
        return (
            rem(hgu_half(ts, g), hgu_half(ts, g), hsend.at[0, ts // CORES], hrecv.at[0, ts // CORES], across),
            rem(hd_half(ts, g), hd_half(ts, g), hsend.at[1, ts // CORES], hrecv.at[1, ts // CORES], across),
        )

    def held_across(ts, gg):
        return (
            rem(hgu_half(ts, gg), hgu_half(ts, gg), hsend.at[2, ts // CORES], hrecv.at[2, ts // CORES], across),
            rem(hd_half(ts, gg), hd_half(ts, gg), hsend.at[3, ts // CORES], hrecv.at[3, ts // CORES], across),
        )

    def held_core(ts):
        return (
            rem(hgu_at(ts), hgu_at(ts), hsend.at[4, ts // CORES], hrecv.at[4, ts // CORES], partner),
            rem(hd_at(ts), hd_at(ts), hsend.at[5, ts // CORES], hrecv.at[5, ts // CORES], partner),
        )

    def a_z(p, up):
        s = slot(p, c, x)
        return rem(
            tok.at[s],
            tok.at[s],
            azsend.at[0 if up else 1, p],
            arecv.at[s],
            dev(z + 1 if up else z - 1, t),
        )

    def a_x(p, k):
        s = slot(p, c, x)
        return rem(tok.at[s], tok.at[s], axsend.at[p], arecv.at[s], xdev(k))

    def a_core(p, xb):
        s = slot(p, c, xb)
        return rem(tok.at[s], tok.at[s], acsend.at[p], arecv.at[s], partner)

    def a_wait(s):
        rem(tok.at[s], tok.at[s], acsend.at[0], arecv.at[s], partner).wait_recv()

    def a_cross(p):
        for k in range(1, xc):
            xb = lax.rem(x + k, xc)
            a_wait(slot(p, c, xb))
            a_core(p, xb).start()

    def r_core(p, xb):
        return rem(
            part.at[slot(p, 1 - c, xb)],
            rd.at[p * xc + xb],
            rdsend.at[p],
            rdrecv.at[p, xb],
            partner,
        )

    piece = rows // PIECES

    def band_of(f):
        return pl.ds(al(f * piece, piece), piece)

    def r_x(p, k, f):
        xb = lax.rem(x + k, xc)
        return rem(
            part.at[slot(p, c, xb), band_of(f)],
            rx.at[p * (xc - 1) + k - 1, band_of(f)],
            rxsend.at[p],
            rxrecv.at[p * (xc - 1) + k - 1, f],
            xdev(k),
        )

    def r_z(p, f):
        return rem(
            part.at[slot(p, c, x), band_of(f)],
            rz.at[z, band_of(f)],
            rzsend.at[p],
            rzrecv.at[z, f],
            dev(p, t),
        )

    near = jnp.where(z == 0, 1, nz - 2)

    def r_relay(p, f):
        return rem(
            part.at[slot(p, c, x), band_of(f)],
            ry.at[p, band_of(f)],
            rzsend.at[p],
            ryrecv.at[p, f],
            dev(near, t),
        )

    def relayed(p):
        return ((z == 1) & (p > 1)) | ((z == nz - 2) & (p < nz - 2))

    @pl.loop(1, nt)
    def _(k):
        for cp in w_out(z * nt + lax.rem(t + k, nt)):
            cp.start()

    for cp in w_mate():
        cp.start()

    @pl.when(z < nz - 1)
    def _():
        a_z(z, True).start()

    @pl.when(z > 0)
    def _():
        a_z(z, False).start()

    a_core(z, x).start()
    for k in range(1, xc):
        a_x(z, k).start()

    @pl.loop(1, n)
    def _(k):
        share_send(lax.rem(me + k, n)).start()

    def send_when(j, cp):
        @pl.when(j != me)
        def _():
            cp.start()


    edge = (z == 0) | (z == nz - 1)
    low = 2 * z < nz

    @pl.loop(0, nz + 1)
    def _(d):
        @pl.when(~edge & (d == 2))
        def _():
            w_planes_across(
                jnp.where(low, z, nz - 1 - z), lambda i: jnp.where(low, z - 1 - i, z + 1 + i)
            )

        late = edge & (d == nz - 1)

        @pl.when((d > 0) & (z - d >= 0) & ~late)
        def _():
            p = z - d
            a_wait(slot(p, c, x))

            @pl.when(z < nz - 1)
            def _():
                a_z(p, True).start()

            for k in range(1, xc):
                a_x(p, k).start()
            a_core(p, x).start()

        @pl.when((d > 0) & (z + d < nz) & ~late)
        def _():
            p = z + d
            a_wait(slot(p, c, x))

            @pl.when(z > 0)
            def _():
                a_z(p, False).start()

            for k in range(1, xc):
                a_x(p, k).start()
            a_core(p, x).start()

        @pl.when(d == nz - 1)
        def _():
            for send, count in ((sgu_send, nz), (sdn_send, nt)):
                for k in range(count):
                    send_when(*send(k))

            for k in range(1, xc):
                for cp in held_x(k):
                    cp.start()

        @pl.when((edge & (d == 0)) | (~edge & (d == 1)))
        def _():
            @pl.loop(1, nz)
            def _(k):
                @pl.when(z + k < nz)
                def _():
                    w_plane_send(z + k)

                @pl.when(z - k >= 0)
                def _():
                    w_plane_send(z - k)

        @pl.when(d == 1)
        def _():
            @pl.loop(1, nt)
            def _(k):
                s = z * nt + lax.rem(t + k, nt)
                for i, at in ((0, gu_at), (1, dn_at)):
                    rem(at(s, g), at(s, g), ysend.at[0], wrecv.at[i, s], across).wait_recv()

                @pl.when(s != mate)
                def _():
                    for cp in w_across(s, g):
                        cp.start()

        @pl.when(late)
        def _():
            w_planes_across(1, lambda i: near)
            w_planes_across(1, lambda i: nz - 1 - z)
            p = nz - 1 - z
            a_wait(slot(p, c, x))
            for k in range(1, xc):
                a_x(p, k).start()
            a_core(p, x).start()

        @pl.when(~edge & (d == nz))
        def _():
            w_planes_across(
                jnp.where(low, nz - 1 - z, z), lambda i: jnp.where(low, z + 1 + i, z - 1 - i)
            )

        @pl.when(edge & (d == nz))
        def _():
            w_planes_across(nz - 3, lambda i: jnp.where(z == 0, nz - 2 - i, 1 + i))

    tail = jnp.where(low, nz - 1, 0)

    @pl.loop(0, nz)
    def _(k):
        p = lax.rem(z + k, nz)

        @pl.when(p != tail)
        def _():
            a_cross(p)

    for k in range(1, xc):
        ts = lax.rem(x + k, xc) * CORES + c
        for cp in held_x_in(ts):
            cp.wait_recv()
        for cp in held_across(ts, g):
            cp.start()

    @pl.loop(1, n)
    def _(k):
        s = lax.rem(me + n - k, n)
        for cp in w_across(s, 1 - g):
            cp.wait_recv()
        rem(shares.at[s], share.at[s], shsend.at[s], shrecv.at[s], across).wait_recv()

    for k in range(nz):

        @pl.when(k * nt + me // nz != me)
        def _():
            rem(sgu_at(k), sgu_at(k), ssend.at[0, k], srecv.at[0, k], across).wait_recv()

    for k in range(nt):

        @pl.when((me // nt) * nt + k != me)
        def _():
            rem(sdn_at(k), sdn_at(k), ssend.at[1, k], srecv.at[1, k], across).wait_recv()

    out_down = pltpu.make_async_copy(w.at[2, pl.ds(0, inner), :], o_down, osem.at[0])
    out_down.start()
    nt_dims = (((1,), (1,)), ((), ()))

    def compute(p, h, xb):
        at = slot(p, h, xb)
        xs = tok[at]
        gate = lax.dot_general(xs, w[0], nt_dims, preferred_element_type=jnp.float32)
        up = lax.dot_general(xs, w[1], nt_dims, preferred_element_type=jnp.float32)
        hidden = gate / (1.0 + jnp.exp(-gate)) * up
        scale = jnp.transpose(
            jnp.broadcast_to(share[p * nt + xb * CORES + h], (rows, rows))
        )[:, :1]
        col = lax.broadcasted_iota(jnp.int32, hidden.shape, 1)
        hidden = jnp.where(col < inner, hidden * scale, hidden).astype(jnp.bfloat16)
        step = min(512, width)
        for lo in range(0, width, step):
            res = jnp.dot(hidden, w[2, :, lo : lo + step], preferred_element_type=jnp.float32)
            part[at, :, lo : lo + step] = res.astype(jnp.bfloat16)

    def work(p):
        @pl.when(p == tail)
        def _():
            a_cross(p)

        for xb in range(xc):
            a_wait(slot(p, 1 - c, xb))

        @pl.loop(0, 2 * xc)
        def _(j):
            k = lax.rem(j // 2 + 1, xc)
            xb = lax.rem(x + k, xc)
            mine = lax.rem(j, 2)
            compute(p, (1 - c) * (1 - mine) + c * mine, xb)

            @pl.when(mine == 0)
            def _():
                r_core(p, xb).start()

            for k2 in range(1, xc):
                @pl.when((mine == 1) & (k == k2))
                def _():
                    r_core(p, xb).wait_recv()
                    s = slot(p, c, xb)
                    part[s] = (
                        part[s].astype(jnp.float32) + rd[p * xc + xb].astype(jnp.float32)
                    ).astype(jnp.bfloat16)
                    for f in range(PIECES):
                        r_x(p, k2, f).start()

    def settle(p, f):
        s = slot(p, c, x)
        at = band_of(f)

        @pl.when(f == 0)
        def _():
            r_core(p, x).wait_recv()

        acc = part[s, at].astype(jnp.float32) + rd[p * xc + x, at].astype(jnp.float32)
        for k in range(1, xc):
            r_x(p, k, f).wait_recv()
            acc = acc + rx[p * (xc - 1) + k - 1, at].astype(jnp.float32)
        part[s, at] = acc.astype(jnp.bfloat16)

        @pl.when(relayed(p))
        def _():
            r_relay(p, f).wait_recv()
            part[s, at] = (acc + ry[p, at].astype(jnp.float32)).astype(jnp.bfloat16)

    def order(i):
        q = jnp.int32(0)
        for zz, planes in enumerate(plane_orders(nz)):
            for ii, p in enumerate(planes):
                q = jnp.where((z == zz) & (i == ii), p, q)
        return q

    @pl.loop(0, nz)
    def _(i):
        work(order(i))

        @pl.when(i == 0)
        def _():
            for i2 in range(2):
                for lo in range(0, width, 256):
                    flip[i2, lo : lo + 256, :] = jnp.transpose(w[i2, :inner, lo : lo + 256])
            for i2, o_w in enumerate((o_gate, o_up)):
                pltpu.make_async_copy(flip.at[i2], o_w, osem.at[1 + i2]).start()

        @pl.when(i > 0)
        def _():
            p = order(i - 1)

            @pl.loop(0, PIECES)
            def _(f):
                settle(p, f)

                @pl.when(edge & (p != near))
                def _():
                    r_relay(p, f).start()

                @pl.when(~edge | (p == near))
                def _():
                    r_z(p, f).start()

    for k in range(1, xc):
        ts = lax.rem(x + k, xc) * CORES + c
        for cp in held_across(ts, 1 - g):
            cp.wait_recv()
    for xb in range(xc):
        for cp in held_core(xb * CORES + c):
            cp.start()
    for xb in range(xc):
        for cp in held_core(xb * CORES + 1 - c):
            cp.wait_recv()
    for i in range(2):
        hflip[i] = jnp.transpose(hgu[i])
    out_held = [
        pltpu.make_async_copy(hflip.at[0], o_hgate, osem.at[3]),
        pltpu.make_async_copy(hflip.at[1], o_hup, osem.at[4]),
        pltpu.make_async_copy(hd, o_hd, osem.at[5 + PIECES]),
    ]
    for cp in out_held:
        cp.start()

    @pl.loop(0, PIECES)
    def _(f):
        at = band_of(f)
        settle(z, f)
        total[at] = part[own, at].astype(jnp.float32)
        for k in range(1, nz):
            zs = lax.rem(z + k, nz)

            @pl.when(((zs > 0) & (zs < nz - 1)) | (zs == z + 1) | (zs == z - 1))
            def _():
                rem(rz.at[zs, at], rz.at[zs, at], rzsend.at[0], rzrecv.at[zs, f], partner).wait_recv()
                total[at] += rz[zs, at].astype(jnp.float32)

        l_tok[at] = total[at].astype(jnp.bfloat16)
        pltpu.make_async_copy(l_tok.at[at], o_mix.at[at], osem.at[5 + f]).start()

    def sent(ref, sem):
        rem(ref, ref, sem, acsend.at[0], partner).wait_send()

    sent(gu.at[:, :, pl.ds(0, half_f), :], wsend.at[0])
    sent(dn.at[:, pl.ds(0, half_r), :], wsend.at[1])
    sent(gu.at[pl.ds(0, n - 2), :, pl.ds(0, half_f), :], ysend.at[0])
    sent(dn.at[pl.ds(0, n - 2), pl.ds(0, half_r), :], ysend.at[1])
    @pl.loop(1, n)
    def _(k):
        share_send(lax.rem(me + k, n)).wait_send()


    for send, count in ((sgu_send, nz), (sdn_send, nt)):
        for k in range(count):
            j, cp = send(k)

            @pl.when(j != me)
            def _():
                cp.wait_send()

    for k in range(1, xc):
        for cp in held_x(k):
            cp.wait_send()
        for cp in held_across(lax.rem(x + k, xc) * CORES + c, g):
            cp.wait_send()
    for xb in range(xc):
        for cp in held_core(xb * CORES + c):
            cp.wait_send()

    @pl.loop(0, nz)
    def _(p):
        @pl.when((p <= z) & (z < nz - 1))
        def _():
            a_z(p, True).wait_send()

        @pl.when((p >= z) & (z > 0))
        def _():
            a_z(p, False).wait_send()

        sent(tok.at[pl.ds(0, xc - 1)], axsend.at[p])
        sent(tok.at[pl.ds(0, xc)], acsend.at[p])
        sent(part.at[pl.ds(0, xc)], rdsend.at[p])
        sent(part.at[pl.ds(0, xc - 1)], rxsend.at[p])

        @pl.when(p != z)
        def _():
            sent(part.at[0], rzsend.at[p])

    out_down.wait()
    for i, o_w in enumerate((o_gate, o_up)):
        pltpu.make_async_copy(flip.at[i], o_w, osem.at[1 + i]).wait()
    for cp in out_held:
        cp.wait()
    for f in range(PIECES):
        pltpu.make_async_copy(l_tok.at[band_of(f)], o_mix.at[band_of(f)], osem.at[5 + f]).wait()


def deliver_kernel(*refs):
    count = (len(refs) - 1) // 3
    src, dst, buf = refs[:count], refs[count : 2 * count], refs[2 * count : 3 * count]
    sems = refs[3 * count]
    for i in range(count):
        pltpu.make_async_copy(src[i], buf[i], sems.at[0, i]).start()
    for i in range(count):
        pltpu.make_async_copy(src[i], buf[i], sems.at[0, i]).wait()
        pltpu.make_async_copy(buf[i], dst[i], sems.at[1, i]).start()
    for i in range(count):
        pltpu.make_async_copy(buf[i], dst[i], sems.at[1, i]).wait()


def deliver(arrays):
    hbm = pl.BlockSpec(memory_space=pltpu.HBM)
    count = len(arrays)
    return pl.pallas_call(
        deliver_kernel,
        out_shape=tuple(jax.ShapeDtypeStruct(a.shape, a.dtype) for a in arrays),
        in_specs=[hbm] * count,
        out_specs=(hbm,) * count,
        scratch_shapes=[pltpu.VMEM(a.shape, a.dtype) for a in arrays]
        + [pltpu.SemaphoreType.DMA((2, count))],
    )(*arrays)


def kernel_plan(
    tokens,
    route_ids,
    route_scores,
    norm_gain,
    expert_gate,
    expert_up,
    expert_down,
    shared_gate,
    shared_up,
    shared_down,
):
    nz = lax.axis_size("fs")
    nt = lax.axis_size("tp")
    n = nz * nt
    xc = nt // CORES
    rows, width = tokens.shape
    picks = route_ids.shape[1]
    dt, ft = expert_gate.shape[1:]
    fr, dc = expert_down.shape[1:]
    st, sr = shared_gate.shape[1], shared_down.shape[0]
    inner = ft * nt
    sd = st * nt // n
    bf, f4 = jnp.bfloat16, jnp.float32
    dma = pltpu.SemaphoreType.DMA
    hbm = pl.BlockSpec(memory_space=pltpu.HBM)
    outs = (
        (rows, width),
        (width, inner),
        (width, inner),
        (inner, width),
        (dt, st * nt),
        (dt, st * nt),
        (sr, width),
    )
    made = pl.pallas_call(
        functools.partial(handover_kernel, nz, nt),
        out_shape=tuple(jax.ShapeDtypeStruct(s, bf) for s in outs),
        in_specs=[hbm] * 10,
        out_specs=(hbm,) * len(outs),
        scratch_shapes=[
            pltpu.VMEM((rows, width), bf),
            pltpu.VMEM((picks, rows), jnp.int32),
            pltpu.VMEM((picks, rows), f4),
            pltpu.VMEM((1, dt), f4),
            pltpu.VMEM((n, ft, dt), f4),
            pltpu.VMEM((n, ft, dt), f4),
            pltpu.VMEM((n, fr, dc), f4),
            pltpu.VMEM((st, dt), f4),
            pltpu.VMEM((st, dt), f4),
            pltpu.VMEM((sr, dc), f4),
            pltpu.VMEM((n, 2, ft, dt), bf),
            pltpu.VMEM((n, fr, dc), bf),
            pltpu.VMEM((2, st, dt), bf),
            pltpu.VMEM((sr, dc), bf),
            pltpu.VMEM((n, 1, rows), f4),
            pltpu.VMEM((3, inner + sd, width), bf),
            pltpu.VMEM((n, rows, width), bf),
            pltpu.VMEM((n, rows, width), bf),
            pltpu.VMEM((nz * xc, rows, width), bf),
            pltpu.VMEM((nz * (xc - 1), rows, width), bf),
            pltpu.VMEM((nz, rows, width), bf),
            pltpu.VMEM((nz, rows, width), bf),
            pltpu.VMEM((rows, width), f4),
            pltpu.VMEM((n, 1, rows), f4),
            pltpu.VMEM((2, st * nt, dt), bf),
            pltpu.VMEM((sr, width), bf),
            pltpu.VMEM((2, width, inner), bf),
            pltpu.VMEM((2, dt, st * nt), bf),
            dma((10,)),
            dma((6 + PIECES,)),
            dma((2,)),
            dma((2, n)),
            dma((2,)),
            dma((2, n)),
            dma((n,)),
            dma((n,)),
            dma((2, max(nz, nt))),
            dma((2, max(nz, nt))),
            dma((6, xc)),
            dma((6, xc)),
            dma((2, nz)),
            dma((nz,)),
            dma((nz,)),
            dma((n,)),
            dma((nz,)),
            dma((nz, xc)),
            dma((nz,)),
            dma((nz * (xc - 1), PIECES)),
            dma((nz,)),
            dma((nz, PIECES)),
            dma((nz, PIECES)),
        ],
        compiler_params=pltpu.CompilerParams(
            collective_id=0, has_side_effects=True, vmem_limit_bytes=60 << 20
        ),
    )(
        tokens,
        route_ids.T,
        route_scores.T,
        norm_gain[None],
        jnp.swapaxes(expert_gate, 1, 2),
        jnp.swapaxes(expert_up, 1, 2),
        expert_down,
        shared_gate.T,
        shared_up.T,
        shared_down,
    )
    mixed, gate, up, down, hgate, hup, hd = deliver(made)
    return mixed, gate[None], up[None], down[None], hgate, hup, hd


def on_device(*args):
    experts = lax.axis_size("fs") * lax.axis_size("tp")
    picks = args[1].shape[1]
    if experts <= 4 * picks:
        return kernel_plan(*args)
    return dispatch_plan(*args)


def solution(mesh):
    return jax.shard_map(
        on_device,
        mesh=mesh,
        in_specs=(
            P(("grp", "fs", "tp"), None),
            P(("grp", "fs", "tp"), None),
            P(("grp", "fs", "tp"), None),
            P("fs"),
            P(None, "fs", "tp"),
            P(None, "fs", "tp"),
            P(None, "fs", "tp"),
            P("fs", "tp"),
            P("fs", "tp"),
            P("fs", "tp"),
        ),
        out_specs=(
            P(("grp", "fs", "tp"), None),
            P(("grp", "fs", "tp"), None, None),
            P(("grp", "fs", "tp"), None, None),
            P(("grp", "fs", "tp"), None, None),
            P(("grp", "fs"), None),
            P(("grp", "fs"), None),
            P(("grp", "fs"), None),
        ),
        check_vma=False,
    )
```

```python
import functools
import jax
import jax.numpy as jnp
from jax import lax
from jax.experimental import pallas as pl
from jax.experimental.pallas import tpu as pltpu
from jax.sharding import PartitionSpec as P

EPSILON = 1e-06
route_scale = 2.5
CORES = 2
PIECES = 4
MESH = pl.DeviceIdType.MESH


def expert_rows(row_block, w_gate, w_up, w_down):
    gate_rows = jnp.dot(row_block, w_gate, preferred_element_type=jnp.float32)
    up_rows = jnp.dot(row_block, w_up, preferred_element_type=jnp.float32)
    hidden = (jax.nn.silu(gate_rows) * up_rows).astype(jnp.bfloat16)
    return jnp.dot(hidden, w_down, preferred_element_type=jnp.float32).astype(jnp.bfloat16)


def relayout(arrived, fs_count, tp_count):
    tile_rows = arrived.shape[2]
    tile_cols = arrived.shape[3]
    grid = arrived.reshape(fs_count, tp_count, tile_rows, tile_cols)
    grid = jnp.transpose(grid, (0, 2, 1, 3))
    return grid.reshape(1, fs_count * tile_rows, tp_count * tile_cols)


def dispatch_plan(
    tokens,
    route_ids,
    route_scores,
    norm_gain,
    expert_gate,
    expert_up,
    expert_down,
    shared_gate,
    shared_up,
    shared_down,
):
    fs_count = lax.axis_size("fs")
    tp_count = lax.axis_size("tp")
    experts = fs_count * tp_count
    gain_col = norm_gain[:, None]
    piece_gate = (gain_col[None] * expert_gate).astype(jnp.bfloat16)
    piece_up = (gain_col[None] * expert_up).astype(jnp.bfloat16)
    piece_down = expert_down.astype(jnp.bfloat16)
    moved = (
        lax.all_to_all(piece_gate[:, None], ("fs", "tp"), split_axis=0, concat_axis=1, tiled=True),
        lax.all_to_all(piece_up[:, None], ("fs", "tp"), split_axis=0, concat_axis=1, tiled=True),
        lax.all_to_all(piece_down[:, None], ("fs", "tp"), split_axis=0, concat_axis=1, tiled=True),
    )
    served_gate = relayout(moved[0], fs_count, tp_count)
    served_up = relayout(moved[1], fs_count, tp_count)
    served_down = relayout(moved[2], fs_count, tp_count)
    tile_gate = (gain_col * shared_gate).astype(jnp.bfloat16)
    tile_up = (gain_col * shared_up).astype(jnp.bfloat16)
    tile_down = shared_down.astype(jnp.bfloat16)
    held_gate, held_up, held_down = (
        lax.all_gather(tile_gate, "tp", axis=1, tiled=True),
        lax.all_gather(tile_up, "tp", axis=1, tiled=True),
        lax.all_gather(tile_down, "tp", axis=1, tiled=True),
    )
    rows_dev = tokens.shape[0]
    width = tokens.shape[1]
    picks = route_ids.shape[1]
    capacity = 3 * rows_dev * picks // (2 * experts)
    widened = tokens.astype(jnp.float32)
    normed = (
        widened * lax.rsqrt(jnp.mean(widened * widened, axis=1, keepdims=True) + EPSILON)
    ).astype(jnp.bfloat16)
    weights = route_scale * route_scores / jnp.sum(route_scores, axis=1, keepdims=True)
    flat_ids = route_ids.reshape(-1)
    onehot = (flat_ids[:, None] == jnp.arange(experts, dtype=jnp.int32)[None, :]).astype(jnp.int32)
    earlier = jnp.cumsum(onehot, axis=0) - onehot
    ranks = jnp.sum(earlier * onehot, axis=1)
    target = flat_ids * capacity + ranks
    outbox = (
        jnp.zeros((experts * capacity, width), jnp.bfloat16)
        .at[target]
        .set(jnp.repeat(normed, picks, axis=0))
    )
    arrived = lax.all_to_all(
        outbox.reshape(experts, capacity, width),
        ("fs", "tp"),
        split_axis=0,
        concat_axis=0,
        tiled=True,
    )
    finished = expert_rows(
        arrived.reshape(-1, width), served_gate[0], served_up[0], served_down[0]
    ).reshape(arrived.shape)
    returned = lax.all_to_all(finished, ("fs", "tp"), split_axis=0, concat_axis=0, tiled=True)
    results = returned.reshape(experts * capacity, width)[target]
    routed = jnp.sum(
        results.reshape(rows_dev, picks, width).astype(jnp.float32) * weights[:, :, None], axis=1
    )
    columns = normed
    gate_part = jnp.dot(
        columns,
        lax.all_gather(held_gate, "fs", axis=0, tiled=True),
        preferred_element_type=jnp.float32,
    )
    up_part = jnp.dot(
        columns,
        lax.all_gather(held_up, "fs", axis=0, tiled=True),
        preferred_element_type=jnp.float32,
    )
    shared_hidden = (jax.nn.silu(gate_part) * up_part).astype(jnp.bfloat16)
    columns = shared_hidden
    shared_term = jnp.dot(
        columns,
        lax.all_gather(held_down, "fs", axis=0, tiled=True),
        preferred_element_type=jnp.float32,
    )
    mixed = (routed + shared_term).astype(jnp.bfloat16)
    return (mixed, served_gate, served_up, served_down, held_gate, held_up, held_down)


def plane_orders(nz):
    orders = []
    for z in range(nz):
        low = 2 * z < nz
        q = z if low else nz - 1 - z
        first = [1] if q == 0 else [0]
        far = [p for p in range(nz - 1, 0, -1) if p != q and p not in first]
        planes = first + (far + [q] if q == 0 else [q] + far)
        orders.append(planes if low else [nz - 1 - p for p in planes])
    return orders


def handover_kernel(
    nz,
    nt,
    tokens,
    ids,
    scores,
    gain,
    in_gate,
    in_up,
    in_down,
    in_sgate,
    in_sup,
    in_sdown,
    o_mix,
    o_gate,
    o_up,
    o_down,
    o_hgate,
    o_hup,
    o_hd,
    l_tok,
    l_ids,
    l_scores,
    l_gain,
    l_gate,
    l_up,
    l_down,
    l_sgate,
    l_sup,
    l_sdown,
    gu,
    dn,
    sgu,
    sdn,
    shares,
    w,
    tok,
    part,
    rd,
    rx,
    rz,
    ry,
    rp,
    total,
    share,
    hgu,
    hd,
    flip,
    hflip,
    lsem,
    osem,
    wsend,
    wrecv,
    ysend,
    yrecv,
    shsend,
    shrecv,
    ssend,
    srecv,
    hsend,
    hrecv,
    azsend,
    axsend,
    acsend,
    arecv,
    rdsend,
    rdrecv,
    rxsend,
    rxrecv,
    rzsend,
    rzrecv,
    ryrecv,
    rpsend,
    rprecv,
):
    n = nz * nt
    xc = nt // CORES
    g = lax.axis_index("grp")
    z = lax.axis_index("fs")
    t = lax.axis_index("tp")
    x = t // CORES
    c = t % CORES
    me = z * nt + t
    rows, width = tokens.shape
    ft, dt = in_gate.shape[1], in_gate.shape[2]
    fr, dc = in_down.shape[1], in_down.shape[2]
    st, sr = in_sgate.shape[0], in_sdown.shape[0]
    inner = ft * nt
    sd = w.shape[1] - inner
    half_f, half_r, half_st, half_sr = ft // 2, fr // 2, st // 2, sr // 2

    def dev(zz, tt, gg=None):
        return {"grp": g if gg is None else gg, "fs": zz, "tp": tt}

    def rem(src, dst, ssem, rsem, device):
        return pltpu.make_async_remote_copy(
            src_ref=src,
            dst_ref=dst,
            send_sem=ssem,
            recv_sem=rsem,
            device_id=device,
            device_id_type=MESH,
        )

    def al(v, m):
        return pl.multiple_of(v, m)

    partner = dev(z, x * CORES + 1 - c)
    across = dev(z, t, 1 - g)
    mate = z * nt + x * CORES + 1 - c

    def xdev(k):
        return dev(z, lax.rem(x + k, xc) * CORES + c)

    def slot(p, h, xb):
        return p * nt + h * xc + xb

    own = slot(z, c, x)

    barrier = pltpu.get_barrier_semaphore()

    @pl.loop(1, n)
    def _(k):
        j = lax.rem(me + k, n)
        pl.semaphore_signal(barrier, 1, device_id=dev(j // nt, j % nt), device_id_type=MESH)

    pl.semaphore_signal(barrier, 1, device_id=across, device_id_type=MESH)

    loads = [
        pltpu.make_async_copy(src, dst, lsem.at[i])
        for i, (src, dst) in enumerate(
            (
                (tokens, l_tok),
                (gain, l_gain),
                (in_gate, l_gate),
                (in_up, l_up),
                (in_down, l_down),
                (in_sgate, l_sgate),
                (in_sup, l_sup),
                (in_sdown, l_sdown),
                (ids, l_ids),
                (scores, l_scores),
            )
        )
    ]
    for cp in loads:
        cp.start()
    loads[0].wait()
    band = min(32, rows)

    @pl.loop(0, rows // band)
    def _(r):
        at = pl.ds(al(r * band, band), band)
        wide = l_tok[at, :].astype(jnp.float32)
        mean = jnp.mean(wide * wide, axis=1, keepdims=True)
        tok[own, at, :] = (wide * lax.rsqrt(mean + EPSILON)).astype(jnp.bfloat16)

    for cp in loads[1:]:
        cp.wait()

    @pl.loop(0, n)
    def _(e):
        gu[e, 0] = (l_gain[...] * l_gate[e]).astype(jnp.bfloat16)
        gu[e, 1] = (l_gain[...] * l_up[e]).astype(jnp.bfloat16)
        dn[e] = l_down[e].astype(jnp.bfloat16)

    sgu[0] = (l_gain[...] * l_sgate[...]).astype(jnp.bfloat16)
    sgu[1] = (l_gain[...] * l_sup[...]).astype(jnp.bfloat16)
    sdn[...] = l_sdown[...].astype(jnp.bfloat16)
    sc = l_scores[...]
    mixing = route_scale * sc / jnp.sum(sc, axis=0, keepdims=True)
    for e in range(n):
        shares[e] = jnp.sum(jnp.where(l_ids[...] == e, mixing, 0.0), axis=0, keepdims=True)
    own_gu = (pl.ds(0, 2), pl.ds(al(t * ft, ft), ft), pl.ds(al(z * dt, dt), dt))
    w[own_gu] = gu[me]
    w[2, pl.ds(al(z * fr, fr), fr), pl.ds(al(t * dc, dc), dc)] = dn[me]
    hgu[:, pl.ds(al(t * st, st), st), :] = sgu[...]
    hd[:, pl.ds(al(t * dc, dc), dc)] = sdn[...]
    share[me] = shares[me]

    @pl.when(me // nz == t)
    def _():
        w[pl.ds(0, 2), pl.ds(inner, sd), pl.ds(al(z * dt, dt), dt)] = sgu[
            :, pl.ds(al((me % nz) * sd, sd), sd), :
        ]

    @pl.when(me // nt == z)
    def _():
        w[2, pl.ds(inner, sd), pl.ds(al(t * dc, dc), dc)] = sdn[
            pl.ds(al((me % nt) * sd, sd), sd), :
        ]

    pl.semaphore_wait(barrier, n)

    def gu_at(src, gg):
        zs, ts = src // nt, src % nt
        return w.at[
            pl.ds(0, 2), pl.ds(al(ts * ft + gg * half_f, half_f), half_f), pl.ds(al(zs * dt, dt), dt)
        ]

    def dn_at(src, gg):
        zs, ts = src // nt, src % nt
        return w.at[2, pl.ds(al(zs * fr + gg * half_r, half_r), half_r), pl.ds(al(ts * dc, dc), dc)]

    def w_send(j, gg, rsems):
        device = dev(j // nt, j % nt)
        return (
            rem(
                gu.at[j, pl.ds(0, 2), pl.ds(al(gg * half_f, half_f), half_f), :],
                gu_at(me, gg),
                wsend.at[0],
                rsems[0],
                device,
            ),
            rem(
                dn.at[j, pl.ds(al(gg * half_r, half_r), half_r), :],
                dn_at(me, gg),
                wsend.at[1],
                rsems[1],
                device,
            ),
        )

    def w_out(j):
        return w_send(j, g, (wrecv.at[0, me], wrecv.at[1, me]))

    def w_mate():
        return w_send(mate, 1 - g, (yrecv.at[0], yrecv.at[1]))

    def w_across(s, gg):
        return (
            rem(gu_at(s, gg), gu_at(s, gg), ysend.at[0], yrecv.at[0], across),
            rem(dn_at(s, gg), dn_at(s, gg), ysend.at[1], yrecv.at[1], across),
        )

    def w_plane_send(p):
        @pl.loop(0, nt)
        def _(k):
            for cp in w_out(p * nt + lax.rem(t + k, nt)):
                cp.start()

    def w_planes_across(count, plane):
        @pl.loop(0, nt)
        def _(k):
            @pl.loop(0, count)
            def _(i):
                s = plane(i) * nt + lax.rem(t + nt - k, nt)
                for m, at in ((0, gu_at), (1, dn_at)):
                    rem(at(s, g), at(s, g), ysend.at[0], wrecv.at[m, s], across).wait_recv()
                for cp in w_across(s, g):
                    cp.start()

    def share_send(j):
        return rem(shares.at[j], share.at[me], shsend.at[j], shrecv.at[me], dev(j // nt, j % nt))

    def sgu_at(zs):
        return w.at[pl.ds(0, 2), pl.ds(inner, sd), pl.ds(al(zs * dt, dt), dt)]

    def sdn_at(ts):
        return w.at[2, pl.ds(inner, sd), pl.ds(al(ts * dc, dc), dc)]

    def sgu_send(k):
        j = t * nz + k
        return j, rem(
            sgu.at[pl.ds(0, 2), pl.ds(k * sd, sd), :],
            sgu_at(z),
            ssend.at[0, k],
            srecv.at[0, z],
            dev(j // nt, j % nt),
        )

    def sdn_send(k):
        j = z * nt + k
        return j, rem(
            sdn.at[pl.ds(k * sd, sd), :],
            sdn_at(t),
            ssend.at[1, k],
            srecv.at[1, t],
            dev(j // nt, j % nt),
        )

    def hgu_half(ts, gg):
        return hgu.at[pl.ds(0, 2), pl.ds(al(ts * st + gg * half_st, half_st), half_st), :]

    def hd_half(ts, gg):
        return hd.at[pl.ds(al(gg * half_sr, half_sr), half_sr), pl.ds(al(ts * dc, dc), dc)]

    def hgu_at(ts):
        return hgu.at[pl.ds(0, 2), pl.ds(al(ts * st, st), st), :]

    def hd_at(ts):
        return hd.at[:, pl.ds(al(ts * dc, dc), dc)]

    def held_x(k):
        return (
            rem(
                sgu.at[pl.ds(0, 2), pl.ds(al(g * half_st, half_st), half_st), :],
                hgu_half(t, g),
                hsend.at[0, x],
                hrecv.at[0, x],
                xdev(k),
            ),
            rem(
                sdn.at[pl.ds(al(g * half_sr, half_sr), half_sr), :],
                hd_half(t, g),
                hsend.at[1, x],
                hrecv.at[1, x],
                xdev(k),
            ),
        )

    def held_x_in(ts):
        return (
            rem(hgu_half(ts, g), hgu_half(ts, g), hsend.at[0, ts // CORES], hrecv.at[0, ts // CORES], across),
            rem(hd_half(ts, g), hd_half(ts, g), hsend.at[1, ts // CORES], hrecv.at[1, ts // CORES], across),
        )

    def held_across(ts, gg):
        return (
            rem(hgu_half(ts, gg), hgu_half(ts, gg), hsend.at[2, ts // CORES], hrecv.at[2, ts // CORES], across),
            rem(hd_half(ts, gg), hd_half(ts, gg), hsend.at[3, ts // CORES], hrecv.at[3, ts // CORES], across),
        )

    def held_core(ts):
        return (
            rem(hgu_at(ts), hgu_at(ts), hsend.at[4, ts // CORES], hrecv.at[4, ts // CORES], partner),
            rem(hd_at(ts), hd_at(ts), hsend.at[5, ts // CORES], hrecv.at[5, ts // CORES], partner),
        )

    def a_z(p, up):
        s = slot(p, c, x)
        return rem(
            tok.at[s],
            tok.at[s],
            azsend.at[0 if up else 1, p],
            arecv.at[s],
            dev(z + 1 if up else z - 1, t),
        )

    def a_x(p, k):
        s = slot(p, c, x)
        return rem(tok.at[s], tok.at[s], axsend.at[p], arecv.at[s], xdev(k))

    def a_core(p, xb):
        s = slot(p, c, xb)
        return rem(tok.at[s], tok.at[s], acsend.at[p], arecv.at[s], partner)

    def a_wait(s):
        rem(tok.at[s], tok.at[s], acsend.at[0], arecv.at[s], partner).wait_recv()

    def a_cross(p):
        for k in range(1, xc):
            xb = lax.rem(x + k, xc)
            a_wait(slot(p, c, xb))
            a_core(p, xb).start()

    def r_core(p, xb):
        return rem(
            part.at[slot(p, 1 - c, xb)],
            rd.at[p * xc + xb],
            rdsend.at[p],
            rdrecv.at[p, xb],
            partner,
        )

    piece = rows // PIECES

    def band_of(f):
        return pl.ds(al(f * piece, piece), piece)

    def r_x(p, k, f):
        xb = lax.rem(x + k, xc)
        return rem(
            part.at[slot(p, c, xb), band_of(f)],
            rx.at[p * (xc - 1) + k - 1, band_of(f)],
            rxsend.at[p],
            rxrecv.at[p * (xc - 1) + k - 1, f],
            xdev(k),
        )

    def r_z(p, f):
        return rem(
            part.at[slot(p, c, x), band_of(f)],
            rz.at[z, band_of(f)],
            rzsend.at[p],
            rzrecv.at[z, f],
            dev(p, t),
        )

    near = jnp.where(z == 0, 1, nz - 2)

    def r_relay(p, f):
        return rem(
            part.at[slot(p, c, x), band_of(f)],
            ry.at[p, band_of(f)],
            rzsend.at[p],
            ryrecv.at[p, f],
            dev(near, t),
        )

    first = PIECES // 2 if nz != 3 else 0
    pair = jnp.where(
        (z == 0) | (z == nz - 1), near, jnp.where(z == 1, 0, jnp.where(z == nz - 2, nz - 1, -1))
    )
    if first == 0:
        pair = jnp.int32(-1)

    def r_pair(k, f):
        xb = lax.rem(x + k, xc)
        return rem(
            part.at[slot(pair, c, xb), band_of(f)],
            rp.at[k - 1, band_of(f)],
            rpsend,
            rprecv.at[k - 1, f],
            dev(pair, t),
        )

    def relayed(p):
        return ((z == 1) & (p > 1)) | ((z == nz - 2) & (p < nz - 2))

    @pl.loop(1, nt)
    def _(k):
        for cp in w_out(z * nt + lax.rem(t + k, nt)):
            cp.start()

    for cp in w_mate():
        cp.start()

    @pl.when(z < nz - 1)
    def _():
        a_z(z, True).start()

    @pl.when(z > 0)
    def _():
        a_z(z, False).start()

    a_core(z, x).start()
    for k in range(1, xc):
        a_x(z, k).start()

    @pl.loop(1, n)
    def _(k):
        share_send(lax.rem(me + k, n)).start()

    def send_when(j, cp):
        @pl.when(j != me)
        def _():
            cp.start()


    edge = (z == 0) | (z == nz - 1)
    low = 2 * z < nz

    @pl.loop(0, nz + 1)
    def _(d):
        @pl.when(~edge & (d == 2))
        def _():
            w_planes_across(
                jnp.where(low, z, nz - 1 - z), lambda i: jnp.where(low, z - 1 - i, z + 1 + i)
            )

        late = edge & (d == nz - 1)

        @pl.when((d > 0) & (z - d >= 0) & ~late)
        def _():
            p = z - d
            a_wait(slot(p, c, x))

            @pl.when(z < nz - 1)
            def _():
                a_z(p, True).start()

            for k in range(1, xc):
                a_x(p, k).start()
            a_core(p, x).start()

        @pl.when((d > 0) & (z + d < nz) & ~late)
        def _():
            p = z + d
            a_wait(slot(p, c, x))

            @pl.when(z > 0)
            def _():
                a_z(p, False).start()

            for k in range(1, xc):
                a_x(p, k).start()
            a_core(p, x).start()

        @pl.when(d == nz - 1)
        def _():
            for send, count in ((sgu_send, nz), (sdn_send, nt)):
                for k in range(count):
                    send_when(*send(k))

            for k in range(1, xc):
                for cp in held_x(k):
                    cp.start()

        @pl.when((edge & (d == 0)) | (~edge & (d == 1)))
        def _():
            @pl.loop(1, nz)
            def _(k):
                @pl.when(z + k < nz)
                def _():
                    w_plane_send(z + k)

                @pl.when(z - k >= 0)
                def _():
                    w_plane_send(z - k)

        @pl.when(d == 1)
        def _():
            @pl.loop(1, nt)
            def _(k):
                s = z * nt + lax.rem(t + k, nt)
                for i, at in ((0, gu_at), (1, dn_at)):
                    rem(at(s, g), at(s, g), ysend.at[0], wrecv.at[i, s], across).wait_recv()

                @pl.when(s != mate)
                def _():
                    for cp in w_across(s, g):
                        cp.start()

        @pl.when(late)
        def _():
            w_planes_across(1, lambda i: near)
            w_planes_across(1, lambda i: nz - 1 - z)
            w_planes_across(nz - 3, lambda i: jnp.where(z == 0, nz - 2 - i, 1 + i))
            p = nz - 1 - z
            a_wait(slot(p, c, x))
            for k in range(1, xc):
                a_x(p, k).start()
            a_core(p, x).start()

        @pl.when(~edge & (d == nz))
        def _():
            w_planes_across(
                jnp.where(low, nz - 1 - z, z), lambda i: jnp.where(low, z + 1 + i, z - 1 - i)
            )

    tail = jnp.where(low, nz - 1, 0)

    @pl.loop(0, nz)
    def _(k):
        p = lax.rem(z + k, nz)

        @pl.when(p != tail)
        def _():
            a_cross(p)

    for k in range(1, xc):
        ts = lax.rem(x + k, xc) * CORES + c
        for cp in held_x_in(ts):
            cp.wait_recv()
        for cp in held_across(ts, g):
            cp.start()

    others = gu.at[pl.ds(0, n - 1), :, pl.ds(0, half_f), :]
    rem(others, others, ysend.at[0], yrecv.at[0], across).wait_recv()
    others = dn.at[pl.ds(0, n - 1), pl.ds(0, half_r), :]
    rem(others, others, ysend.at[1], yrecv.at[1], across).wait_recv()

    @pl.loop(1, n)
    def _(k):
        s = lax.rem(me + n - k, n)
        rem(shares.at[s], share.at[s], shsend.at[s], shrecv.at[s], across).wait_recv()

    for k in range(nz):

        @pl.when(k * nt + me // nz != me)
        def _():
            rem(sgu_at(k), sgu_at(k), ssend.at[0, k], srecv.at[0, k], across).wait_recv()

    for k in range(nt):

        @pl.when((me // nt) * nt + k != me)
        def _():
            rem(sdn_at(k), sdn_at(k), ssend.at[1, k], srecv.at[1, k], across).wait_recv()

    out_down = pltpu.make_async_copy(w.at[2, pl.ds(0, inner), :], o_down, osem.at[0])
    out_down.start()
    nt_dims = (((1,), (1,)), ((), ()))

    def compute(p, h, xb):
        at = slot(p, h, xb)
        xs = tok[at]
        gate = lax.dot_general(xs, w[0], nt_dims, preferred_element_type=jnp.float32)
        up = lax.dot_general(xs, w[1], nt_dims, preferred_element_type=jnp.float32)
        hidden = gate / (1.0 + jnp.exp(-gate)) * up
        scale = jnp.transpose(
            jnp.broadcast_to(share[p * nt + xb * CORES + h], (rows, rows))
        )[:, :1]
        col = lax.broadcasted_iota(jnp.int32, hidden.shape, 1)
        hidden = jnp.where(col < inner, hidden * scale, hidden).astype(jnp.bfloat16)
        step = min(512, width)
        for lo in range(0, width, step):
            res = jnp.dot(hidden, w[2, :, lo : lo + step], preferred_element_type=jnp.float32)
            part[at, :, lo : lo + step] = res.astype(jnp.bfloat16)

    def work(p):
        @pl.when(p == tail)
        def _():
            a_cross(p)

        for xb in range(xc):
            a_wait(slot(p, 1 - c, xb))

        @pl.loop(0, 2 * xc)
        def _(j):
            k = lax.rem(j // 2 + 1, xc)
            xb = lax.rem(x + k, xc)
            mine = lax.rem(j, 2)
            compute(p, (1 - c) * (1 - mine) + c * mine, xb)

            @pl.when(mine == 0)
            def _():
                r_core(p, xb).start()

            for k2 in range(1, xc):
                @pl.when((mine == 1) & (k == k2))
                def _():
                    r_core(p, xb).wait_recv()
                    s = slot(p, c, xb)
                    part[s] = (
                        part[s].astype(jnp.float32) + rd[p * xc + xb].astype(jnp.float32)
                    ).astype(jnp.bfloat16)
                    for f in range(first, PIECES):
                        r_x(p, k2, f).start()
                    for f in range(first):
                        @pl.when(p == pair)
                        def _():
                            r_pair(k2, f).start()

                        @pl.when((p == z) & (pair >= 0))
                        def _():
                            r_pair(k2, f).wait_recv()
                            at = band_of(f)
                            part[s, at] = (
                                part[s, at].astype(jnp.float32)
                                + rp[k2 - 1, at].astype(jnp.float32)
                            ).astype(jnp.bfloat16)

                        @pl.when(p != pair)
                        def _():
                            r_x(p, k2, f).start()

    def settle(p, turn):
        s = slot(p, c, x)
        f = jnp.where(p == pair, turn, lax.rem(turn + first, PIECES))
        at = band_of(f)

        @pl.when(turn == 0)
        def _():
            r_core(p, x).wait_recv()

        total[at] = part[s, at].astype(jnp.float32) + rd[p * xc + x, at].astype(jnp.float32)

        @pl.when((p != pair) | (f >= first))
        def _():
            for k in range(1, xc):
                r_x(p, k, f).wait_recv()
                total[at] += rx[p * (xc - 1) + k - 1, at].astype(jnp.float32)

        @pl.when(relayed(p))
        def _():
            r_relay(p, f).wait_recv()
            total[at] += ry[p, at].astype(jnp.float32)

        return f, at

    def order(i):
        q = jnp.int32(0)
        for zz, planes in enumerate(plane_orders(nz)):
            for ii, p in enumerate(planes):
                q = jnp.where((z == zz) & (i == ii), p, q)
        return q

    def emit(p, turn):
        f, at = settle(p, turn)
        part[slot(p, c, x), at] = total[at].astype(jnp.bfloat16)

        @pl.when(edge & (p != near))
        def _():
            r_relay(p, f).start()

        @pl.when(~edge | (p == near))
        def _():
            r_z(p, f).start()

    def emit_rest(p):
        @pl.when(p != z)
        def _():
            @pl.loop(jnp.where(p == pair, first, 0), PIECES)
            def _(turn):
                emit(p, turn)

    @pl.loop(0, nz)
    def _(i):
        work(order(i))

        @pl.when((i == 0) & (pair >= 0))
        def _():
            @pl.loop(0, first)
            def _(turn):
                emit(pair, turn)

        @pl.when(i == 0)
        def _():
            for i2 in range(2):
                for lo in range(0, width, 256):
                    flip[i2, lo : lo + 256, :] = jnp.transpose(w[i2, :inner, lo : lo + 256])
            for i2, o_w in enumerate((o_gate, o_up)):
                pltpu.make_async_copy(flip.at[i2], o_w, osem.at[1 + i2]).start()

        @pl.when(i > 0)
        def _():
            emit_rest(order(i - 1))

    emit_rest(order(nz - 1))

    for k in range(1, xc):
        ts = lax.rem(x + k, xc) * CORES + c
        for cp in held_across(ts, 1 - g):
            cp.wait_recv()
    for xb in range(xc):
        for cp in held_core(xb * CORES + c):
            cp.start()
    for xb in range(xc):
        for cp in held_core(xb * CORES + 1 - c):
            cp.wait_recv()
    for i in range(2):
        hflip[i] = jnp.transpose(hgu[i])
    out_held = [
        pltpu.make_async_copy(hflip.at[0], o_hgate, osem.at[3]),
        pltpu.make_async_copy(hflip.at[1], o_hup, osem.at[4]),
        pltpu.make_async_copy(hd, o_hd, osem.at[5 + PIECES]),
    ]
    for cp in out_held:
        cp.start()

    @pl.loop(0, PIECES)
    def _(turn):
        f, at = settle(z, turn)
        for k in range(1, nz):
            zs = lax.rem(z + k, nz)

            @pl.when(((zs > 0) & (zs < nz - 1)) | (zs == z + 1) | (zs == z - 1))
            def _():
                rem(rz.at[zs, at], rz.at[zs, at], rzsend.at[0], rzrecv.at[zs, f], partner).wait_recv()
                total[at] += rz[zs, at].astype(jnp.float32)

        l_tok[at] = total[at].astype(jnp.bfloat16)
        pltpu.make_async_copy(l_tok.at[at], o_mix.at[at], osem.at[5 + f]).start()

    def sent(ref, sem):
        rem(ref, ref, sem, acsend.at[0], partner).wait_send()

    sent(gu.at[:, :, pl.ds(0, half_f), :], wsend.at[0])
    sent(dn.at[:, pl.ds(0, half_r), :], wsend.at[1])
    sent(gu.at[pl.ds(0, n - 2), :, pl.ds(0, half_f), :], ysend.at[0])
    sent(dn.at[pl.ds(0, n - 2), pl.ds(0, half_r), :], ysend.at[1])
    @pl.loop(1, n)
    def _(k):
        share_send(lax.rem(me + k, n)).wait_send()


    for send, count in ((sgu_send, nz), (sdn_send, nt)):
        for k in range(count):
            j, cp = send(k)

            @pl.when(j != me)
            def _():
                cp.wait_send()

    for k in range(1, xc):
        for cp in held_x(k):
            cp.wait_send()
        for cp in held_across(lax.rem(x + k, xc) * CORES + c, g):
            cp.wait_send()
    for xb in range(xc):
        for cp in held_core(xb * CORES + c):
            cp.wait_send()

    @pl.loop(0, nz)
    def _(p):
        @pl.when((p <= z) & (z < nz - 1))
        def _():
            a_z(p, True).wait_send()

        @pl.when((p >= z) & (z > 0))
        def _():
            a_z(p, False).wait_send()

        sent(tok.at[pl.ds(0, xc - 1)], axsend.at[p])
        sent(tok.at[pl.ds(0, xc)], acsend.at[p])
        sent(part.at[pl.ds(0, xc)], rdsend.at[p])

        @pl.when(p != pair)
        def _():
            sent(part.at[pl.ds(0, xc - 1)], rxsend.at[p])

        if first > 0:
            @pl.when(p == pair)
            def _():
                sent(part.at[pl.ds(0, xc - 1), pl.ds(0, rows - first * piece)], rxsend.at[p])
                sent(part.at[pl.ds(0, xc - 1), pl.ds(0, first * piece)], rpsend)


        @pl.when(p != z)
        def _():
            sent(part.at[0], rzsend.at[p])

    out_down.wait()
    for i, o_w in enumerate((o_gate, o_up)):
        pltpu.make_async_copy(flip.at[i], o_w, osem.at[1 + i]).wait()
    for cp in out_held:
        cp.wait()
    for f in range(PIECES):
        pltpu.make_async_copy(l_tok.at[band_of(f)], o_mix.at[band_of(f)], osem.at[5 + f]).wait()


def deliver_kernel(*refs):
    count = (len(refs) - 1) // 3
    src, dst, buf = refs[:count], refs[count : 2 * count], refs[2 * count : 3 * count]
    sems = refs[3 * count]
    for i in range(count):
        pltpu.make_async_copy(src[i], buf[i], sems.at[0, i]).start()
    for i in range(count):
        pltpu.make_async_copy(src[i], buf[i], sems.at[0, i]).wait()
        pltpu.make_async_copy(buf[i], dst[i], sems.at[1, i]).start()
    for i in range(count):
        pltpu.make_async_copy(buf[i], dst[i], sems.at[1, i]).wait()


def deliver(arrays):
    hbm = pl.BlockSpec(memory_space=pltpu.HBM)
    count = len(arrays)
    return pl.pallas_call(
        deliver_kernel,
        out_shape=tuple(jax.ShapeDtypeStruct(a.shape, a.dtype) for a in arrays),
        in_specs=[hbm] * count,
        out_specs=(hbm,) * count,
        scratch_shapes=[pltpu.VMEM(a.shape, a.dtype) for a in arrays]
        + [pltpu.SemaphoreType.DMA((2, count))],
    )(*arrays)


def kernel_plan(
    tokens,
    route_ids,
    route_scores,
    norm_gain,
    expert_gate,
    expert_up,
    expert_down,
    shared_gate,
    shared_up,
    shared_down,
):
    nz = lax.axis_size("fs")
    nt = lax.axis_size("tp")
    n = nz * nt
    xc = nt // CORES
    rows, width = tokens.shape
    picks = route_ids.shape[1]
    dt, ft = expert_gate.shape[1:]
    fr, dc = expert_down.shape[1:]
    st, sr = shared_gate.shape[1], shared_down.shape[0]
    inner = ft * nt
    sd = st * nt // n
    bf, f4 = jnp.bfloat16, jnp.float32
    dma = pltpu.SemaphoreType.DMA
    hbm = pl.BlockSpec(memory_space=pltpu.HBM)
    outs = (
        (rows, width),
        (width, inner),
        (width, inner),
        (inner, width),
        (dt, st * nt),
        (dt, st * nt),
        (sr, width),
    )
    made = pl.pallas_call(
        functools.partial(handover_kernel, nz, nt),
        out_shape=tuple(jax.ShapeDtypeStruct(s, bf) for s in outs),
        in_specs=[hbm] * 10,
        out_specs=(hbm,) * len(outs),
        scratch_shapes=[
            pltpu.VMEM((rows, width), bf),
            pltpu.VMEM((picks, rows), jnp.int32),
            pltpu.VMEM((picks, rows), f4),
            pltpu.VMEM((1, dt), f4),
            pltpu.VMEM((n, ft, dt), f4),
            pltpu.VMEM((n, ft, dt), f4),
            pltpu.VMEM((n, fr, dc), f4),
            pltpu.VMEM((st, dt), f4),
            pltpu.VMEM((st, dt), f4),
            pltpu.VMEM((sr, dc), f4),
            pltpu.VMEM((n, 2, ft, dt), bf),
            pltpu.VMEM((n, fr, dc), bf),
            pltpu.VMEM((2, st, dt), bf),
            pltpu.VMEM((sr, dc), bf),
            pltpu.VMEM((n, 1, rows), f4),
            pltpu.VMEM((3, inner + sd, width), bf),
            pltpu.VMEM((n, rows, width), bf),
            pltpu.VMEM((n, rows, width), bf),
            pltpu.VMEM((nz * xc, rows, width), bf),
            pltpu.VMEM((nz * (xc - 1), rows, width), bf),
            pltpu.VMEM((nz, rows, width), bf),
            pltpu.VMEM((nz, rows, width), bf),
            pltpu.VMEM((xc - 1, rows, width), bf),
            pltpu.VMEM((rows, width), f4),
            pltpu.VMEM((n, 1, rows), f4),
            pltpu.VMEM((2, st * nt, dt), bf),
            pltpu.VMEM((sr, width), bf),
            pltpu.VMEM((2, width, inner), bf),
            pltpu.VMEM((2, dt, st * nt), bf),
            dma((10,)),
            dma((6 + PIECES,)),
            dma((2,)),
            dma((2, n)),
            dma((2,)),
            dma((2,)),
            dma((n,)),
            dma((n,)),
            dma((2, max(nz, nt))),
            dma((2, max(nz, nt))),
            dma((6, xc)),
            dma((6, xc)),
            dma((2, nz)),
            dma((nz,)),
            dma((nz,)),
            dma((n,)),
            dma((nz,)),
            dma((nz, xc)),
            dma((nz,)),
            dma((nz * (xc - 1), PIECES)),
            dma((nz,)),
            dma((nz, PIECES)),
            dma((nz, PIECES)),
            dma,
            dma((xc - 1, PIECES)),
        ],
        compiler_params=pltpu.CompilerParams(
            collective_id=0, has_side_effects=True, vmem_limit_bytes=60 << 20
        ),
    )(
        tokens,
        route_ids.T,
        route_scores.T,
        norm_gain[None],
        jnp.swapaxes(expert_gate, 1, 2),
        jnp.swapaxes(expert_up, 1, 2),
        expert_down,
        shared_gate.T,
        shared_up.T,
        shared_down,
    )
    mixed, gate, up, down, hgate, hup, hd = deliver(made)
    return mixed, gate[None], up[None], down[None], hgate, hup, hd


def on_device(*args):
    experts = lax.axis_size("fs") * lax.axis_size("tp")
    picks = args[1].shape[1]
    if experts <= 4 * picks:
        return kernel_plan(*args)
    return dispatch_plan(*args)


def solution(mesh):
    return jax.shard_map(
        on_device,
        mesh=mesh,
        in_specs=(
            P(("grp", "fs", "tp"), None),
            P(("grp", "fs", "tp"), None),
            P(("grp", "fs", "tp"), None),
            P("fs"),
            P(None, "fs", "tp"),
            P(None, "fs", "tp"),
            P(None, "fs", "tp"),
            P("fs", "tp"),
            P("fs", "tp"),
            P("fs", "tp"),
        ),
        out_specs=(
            P(("grp", "fs", "tp"), None),
            P(("grp", "fs", "tp"), None, None),
            P(("grp", "fs", "tp"), None, None),
            P(("grp", "fs", "tp"), None, None),
            P(("grp", "fs"), None),
            P(("grp", "fs"), None),
            P(("grp", "fs"), None),
        ),
        check_vma=False,
    )
```
